512 devices in a mesh: ep: 32 (over z, core), tp: 16 (over y, x).
Axes of the slice: x: 4, y: 4, z: 16, core: 2. Of those that a mesh axis runs over, the one named last changes fastest.
Arguments:
- query_maps: bfloat16 [8192, 4096], P('ep', 'tp'), may hold values from -40 to 40
- key_maps: bfloat16 [8192, 4096], P('ep', 'tp'), may hold values from -40 to 40
- value_rows: bfloat16 [8192, 4096], P('ep', 'tp'), may hold values from -6 to 6
- head_lambda: float32 [16], P('tp'), may hold values from 0.3 to 0.8
- head_gain: float32 [256], replicated, may hold values from 0.1 to 1.9
- out_weight: bfloat16 [4096, 2048], P('tp'), may hold values from -0.125 to 0.125
- expert_rows: bfloat16 [4096, 2048], P('ep'), may hold values from -6 to 6
- expert_gain: float32 [2048], replicated, may hold values from 0.1 to 1.9
- routes: int32 [4096, 2], P('ep'), may hold values from 0 to 31, all different within a row; in each aligned block of 128 rows (0 to 127, 128 to 255, ...) at most 12 rows name the same one
- route_weights: float32 [4096, 2], P('ep'), may hold values from 0.2 to 1
- gate_weight: bfloat16 [32, 2048, 4096], P('ep', None, 'tp'), may hold values from -0.125 to 0.125
- up_weight: bfloat16 [32, 2048, 4096], P('ep', None, 'tp'), may hold values from -0.125 to 0.125
- down_weight: bfloat16 [32, 4096, 2048], P('ep', 'tp'), may hold values from -0.125 to 0.125
Outputs:
- mixed: bfloat16 [8192, 2048], P('ep', 'tp')
- expert_out: bfloat16 [4096, 2048], P('ep', 'tp')
The draws below stay inside these ranges and needn't reach their ends.
Inputs may be any that keep to these rules, and one draw needn't show every extreme that they name: `routes`: within the rows of one device (aligned blocks of 128 rows) no expert is named more than 12 times, and the 2 experts of a row differ.
All inputs are finite; a program needn't handle non-finite values.
Results may differ from the reference program's by a relative error of at most 0.018.
Values may be sent and summed in bfloat16 or wider, within the bound.
A program may use at most 128 MiB of HBM per device.

```python
import math
import jax
import jax.numpy as jnp
import numpy as np
from jax import lax

D = 2048
HEADS = 16
HEAD = 128
VHEAD = 256
FF = 4096
TOPK = 2
MOE_DEV = 128
TOKENS = 8192
MOE_TOK = 4096
EXPERTS = 32
CAP = 12
N_EP = 32
N_TP = 16


def draw_query_maps(key, part):
    base = jnp.clip(1.3 * jax.random.normal(jax.random.fold_in(key, 1), (TOKENS, HEADS * 2 * HEAD), jnp.float32), -7.8, 7.8)
    return base.astype(jnp.bfloat16)


def draw_key_maps(key, part):
    base = jnp.clip(1.3 * jax.random.normal(jax.random.fold_in(key, 2), (TOKENS, HEADS * 2 * HEAD), jnp.float32), -7.8, 7.8)
    base = base.reshape(TOKENS, HEADS, 2, HEAD)
    return base.reshape(TOKENS, HEADS * 2 * HEAD).astype(jnp.bfloat16)


def spiked(result, own_key, source, target, shards_of, factor):
    owner, partner = [(jnp.arange(result.shape[axis_at]) // (result.shape[axis_at] // shards_of)).reshape([-1 if axis == axis_at else 1 for axis in range(result.ndim)]) for axis_at in (source, target)]
    chosen = jax.random.permutation(own_key, shards_of)[partner]
    strong = (owner == chosen) | (owner == (partner + shards_of // 2) % shards_of)
    return jnp.where(strong, factor * result, result)


def level_of(stream_key, dims, cuts, low, top_value):
    loudness = 1.0
    for axis_at, blocks in cuts:
        steps = jax.random.uniform(jax.random.fold_in(jax.random.fold_in(stream_key, 6), axis_at), (blocks,), jnp.float32, low / len(cuts), top_value / len(cuts))
        loudness = loudness * jnp.repeat(jnp.exp(steps), dims[axis_at] // blocks).reshape((-1,) + (1,) * (len(dims) - 1 - axis_at))
    return loudness


def routed_block(stream_key, own, number, rows, amount, top, most, skew):
    order = jax.random.permutation(stream_key, amount)
    heavy_load, ordinary = load_shares(amount, rows * top, most, skew, True), load_shares(amount, rows * top, most, skew, False)
    places = jnp.arange(amount)

    def named(sizes, turn):
        used = int((sizes > 0).sum())
        fixed = max(1, used // 4)
        passed = fixed + (places - fixed + turn * (used - fixed)) % max(1, amount - fixed)
        return jnp.zeros((amount,), jnp.int32).at[order[jnp.where(places < fixed, places, passed)]].set(jnp.asarray(sizes, jnp.int32))

    sizes = jnp.where(number % 4 == 0, named(heavy_load, number // 4), named(ordinary, number - number // 4 - 1))
    mixed = jax.random.permutation(jax.random.fold_in(own, 3), amount)
    source_of, receiver = mixed[0:amount // 2 * 2:2], mixed[1:amount // 2 * 2:2]
    room = jnp.minimum(sizes[source_of] - 1, most - sizes[receiver]) // 2
    room = jnp.where((source_of == order[0]) | (receiver == order[0]) | (sizes[receiver] == 0), 0, jnp.maximum(room, 0))
    passed = jax.random.randint(jax.random.fold_in(own, 4), (amount // 2,), 0, 1 << 20) % (room + 1)
    sizes = sizes.at[source_of].add(-passed).at[receiver].add(passed)
    labels = jnp.searchsorted(jnp.cumsum(sizes), jnp.arange(rows * top), side="right").astype(jnp.int32)
    table = labels.reshape(top, rows).T
    table = table[jax.random.permutation(jax.random.fold_in(own, 1), rows)]
    turn = jax.random.randint(jax.random.fold_in(own, 2), (rows, 1), 0, top)
    return jnp.take_along_axis(table, (jnp.arange(top)[None, :] + turn) % top, axis=1)


def load_shares(number_of, total, bound, lean, full):
    portions = [(1 << 20) // math.isqrt(standing ** lean) + 1 for standing in range(1, number_of + 1)]
    largest = bound if full else min(bound, max(-(-total // number_of), total * portions[0] // sum(portions)))
    least = 1 if total - largest >= number_of - 1 else 0
    holding, surplus = [largest] + [least] * (number_of - 1), total - largest - least * (number_of - 1)
    while surplus > 0:
        free = [i for i in range(1, number_of) if holding[i] < largest] or [i for i in range(1, number_of) if holding[i] < bound]
        mass, budget = sum([portions[i] for i in free]), surplus
        for i in free:
            extra = min(bound - holding[i], max(1, budget * portions[i] // mass), surplus)
            holding[i] = holding[i] + extra
            surplus = surplus - extra
    return np.array(holding)


def centred(rng, extent, spread, bound, cuts=(), kind=jnp.bfloat16):
    array = spread * jax.random.normal(rng, extent, jnp.float32)
    if cuts:
        array = array * level_of(rng, extent, cuts, -0.22, 0.18)
    return jnp.clip(array, -bound, bound).astype(kind)


def heavy_noise(rng, extent, scale, most, split, heavy, kind=jnp.bfloat16):
    array = scale * jax.random.normal(rng, extent, jnp.float32)
    if split:
        array = array * level_of(rng, extent, split, -0.22, 0.18)
    return jnp.clip(spiked(array, jax.random.fold_in(rng, 3), *heavy), -most, most).astype(kind)


def setup_inputs(seed: int = 0) -> dict:
    key_list = jax.random.split(jax.random.key(seed), 14)
    query_maps = draw_query_maps(jax.random.fold_in(key_list[13], 71), 0)
    key_maps = draw_key_maps(jax.random.fold_in(key_list[13], 71), 0)
    value_rows = centred(key_list[2], (TOKENS, HEADS * VHEAD), 1.0, 6.0, ((0, 32), (1, 16)))
    head_lambda = jnp.clip(0.3 + 0.5 * jax.random.uniform(key_list[3], (HEADS,), jnp.float32) ** level_of(key_list[3], (HEADS,), ((0, 16),), -0.2, 0.2), 0.3, 0.8)
    head_gain = jnp.clip(1.0 + 0.18 * jax.random.normal(key_list[4], (VHEAD,), jnp.float32), 0.1, 1.9)
    out_weight = heavy_noise(key_list[5], (HEADS * VHEAD, D), (HEADS * VHEAD) ** -0.5, 0.125, ((0, 16),), (0, 1, 16, 2.0))
    expert_rows = centred(key_list[6], (MOE_TOK, D), 1.0, 6.0, ((0, 32),))
    expert_gain = jnp.clip(1.0 + 0.18 * jax.random.normal(key_list[7], (D,), jnp.float32), 0.1, 1.9)
    routes_keys = jax.random.split(jax.random.fold_in(key_list[8], 1), MOE_TOK // MOE_DEV)
    routes_turns = jax.random.permutation(jax.random.fold_in(key_list[8], 3), MOE_TOK // MOE_DEV)
    routes = jax.vmap(lambda own, number: routed_block(jax.random.fold_in(key_list[8], 2), own, number, MOE_DEV, EXPERTS, TOPK, CAP, 2))(routes_keys, routes_turns).reshape((MOE_TOK, TOPK))
    route_weights = jnp.clip(0.2 + 0.8 * jax.random.uniform(key_list[9], (MOE_TOK, TOPK), jnp.float32) ** level_of(key_list[9], (MOE_TOK, TOPK), ((0, 32),), -0.2, 0.2), 0.2, 1.0)
    gate_weight = centred(key_list[10], (EXPERTS, D, FF), D ** -0.5, 0.125, ((0, 32), (2, 16)))
    up_weight = centred(key_list[11], (EXPERTS, D, FF), D ** -0.5, 0.125, ((0, 32), (2, 16)))
    down_weight = heavy_noise(key_list[12], (EXPERTS, FF, D), FF ** -0.5, 0.125, ((0, 32), (1, 16)), (1, 2, 16, 2.0))
    return dict(query_maps=query_maps, key_maps=key_maps, value_rows=value_rows, head_lambda=head_lambda, head_gain=head_gain, out_weight=out_weight, expert_rows=expert_rows, expert_gain=expert_gain, routes=routes, route_weights=route_weights, gate_weight=gate_weight, up_weight=up_weight, down_weight=down_weight)


norm_eps = 1e-06
rope_base = 10000.0

def rope_turn(inputs, positions):
    half_dim = inputs.shape[-1] // 2
    inverse = rope_base ** (-2.0 * jnp.arange(half_dim, dtype=jnp.float32) / inputs.shape[-1])
    angles = positions.astype(jnp.float32)[:, None] * inverse[None, :]
    cos_table = jnp.cos(angles)[:, None, None, :]
    sin_table = jnp.sin(angles)[:, None, None, :]
    first_half = inputs[..., :half_dim]
    second_half = inputs[..., half_dim:]
    return jnp.concatenate([first_half * cos_table - second_half * sin_table, second_half * cos_table + first_half * sin_table], axis=-1)

def mixer_half(query_maps, key_maps, value_rows, head_lambda, head_gain, out_weight):
    positions = jnp.arange(TOKENS, dtype=jnp.int32)
    rotated_q = rope_turn(query_maps.astype(jnp.float32).reshape(TOKENS, HEADS, 2, HEAD), positions).astype(jnp.bfloat16)
    rotated_k = rope_turn(key_maps.astype(jnp.float32).reshape(TOKENS, HEADS, 2, HEAD), positions).astype(jnp.bfloat16)
    values_all = value_rows.reshape(TOKENS, HEADS, VHEAD)
    block_size = math.gcd(512, TOKENS)
    score_scale = HEAD ** (-0.5)

    def one_head(head_index):
        head_q = rotated_q[:, head_index].astype(jnp.float32)
        head_k = rotated_k[:, head_index].astype(jnp.float32)
        head_v = values_all[:, head_index].astype(jnp.float32)
        key_pos = jnp.arange(TOKENS, dtype=jnp.int32)

        def one_block(block_index):
            first_row = (block_index * block_size).astype(jnp.int32)
            block_q = lax.dynamic_slice_in_dim(head_q, first_row, block_size, 0)
            query_pos = first_row + jnp.arange(block_size, dtype=jnp.int32)
            scores = jnp.einsum('qmd,kmd->mqk', block_q, head_k) * score_scale
            causal = (key_pos[None, :] <= query_pos[:, None])[None]
            masked = jnp.where(causal, scores, -jnp.inf)
            peak = lax.optimization_barrier(jnp.max(masked, axis=-1, keepdims=True))
            expd = jnp.where(causal, jnp.exp(masked - peak), 0.0)
            probs = expd / lax.optimization_barrier(jnp.sum(expd, axis=-1, keepdims=True))
            rounded = lax.optimization_barrier(probs.astype(jnp.bfloat16))
            map_out = jnp.einsum('mqk,ke->mqe', rounded.astype(jnp.float32), head_v)
            difference = map_out[0] - head_lambda[head_index] * map_out[1]
            normed = difference * lax.rsqrt(lax.optimization_barrier(jnp.mean(difference * difference, axis=-1, keepdims=True)) + norm_eps) * head_gain
            return normed.astype(jnp.bfloat16)
        blocks = lax.map(one_block, jnp.arange(TOKENS // block_size, dtype=jnp.int32))
        return blocks.reshape(TOKENS, VHEAD)
    per_head = lax.map(one_head, jnp.arange(HEADS, dtype=jnp.int32))
    group_size = HEADS // N_TP
    grouped = per_head.reshape(N_TP, group_size, TOKENS, VHEAD)
    weight_groups = out_weight.reshape(N_TP, group_size, VHEAD, D)

    def add_group(running, pieces):
        group_heads, group_weight = pieces
        partial_value = jnp.einsum('hte,hed->td', group_heads.astype(jnp.float32), group_weight.astype(jnp.float32))
        rounded = lax.optimization_barrier(partial_value.astype(jnp.bfloat16))
        return (running + rounded.astype(jnp.float32), None)
    summed, _ = lax.scan(add_group, jnp.zeros((TOKENS, D), jnp.float32), (grouped, weight_groups))
    return summed.astype(jnp.bfloat16)

def expert_half(expert_rows, expert_gain, routes, route_weights, gate_weight, up_weight, down_weight):
    inputs = expert_rows.astype(jnp.float32)
    normed = (inputs * lax.rsqrt(lax.optimization_barrier(jnp.mean(inputs * inputs, axis=-1, keepdims=True)) + norm_eps) * expert_gain).astype(jnp.bfloat16)
    expert_ids = routes.reshape(N_EP, MOE_DEV * TOPK)
    one_hot = (expert_ids[..., None] == jnp.arange(EXPERTS, dtype=jnp.int32)).astype(jnp.int32)
    slot_index = lax.optimization_barrier(jnp.sum((jnp.cumsum(one_hot, axis=1) - one_hot) * one_hot, axis=-1)).astype(jnp.int32)
    source_block = jnp.zeros_like(expert_ids) + jnp.arange(N_EP, dtype=jnp.int32)[:, None]
    repeated = jnp.repeat(normed.reshape(N_EP, MOE_DEV, D), TOPK, axis=1)
    buffer = jnp.zeros((EXPERTS, N_EP, CAP, D), normed.dtype).at[expert_ids, source_block, slot_index].set(repeated)
    group_width = FF // N_TP

    def run_one(pieces):
        slots, gate_one, up_one, down_one = pieces
        flat_rows = slots.reshape(N_EP * CAP, D)
        gate_values = jnp.dot(flat_rows, gate_one, preferred_element_type=jnp.float32)
        up_values = jnp.dot(flat_rows, up_one, preferred_element_type=jnp.float32)
        hidden = (jax.nn.silu(gate_values) * up_values).astype(jnp.bfloat16)
        hidden_groups = jnp.transpose(hidden.reshape(N_EP * CAP, N_TP, group_width), (1, 0, 2))
        down_groups = down_one.reshape(N_TP, group_width, D)

        def add_group(running, pieces_inner):
            hidden_part, down_part = pieces_inner
            partial_value = jnp.dot(hidden_part, down_part, preferred_element_type=jnp.float32)
            rounded = lax.optimization_barrier(partial_value.astype(jnp.bfloat16))
            return (running + rounded.astype(jnp.float32), None)
        summed, _ = lax.scan(add_group, jnp.zeros((N_EP * CAP, D), jnp.float32), (hidden_groups, down_groups))
        return summed.astype(jnp.bfloat16).reshape(N_EP, CAP, D)
    results = lax.map(run_one, (buffer, gate_weight, up_weight, down_weight))
    picked = results[expert_ids, source_block, slot_index].reshape(MOE_TOK, TOPK, D)
    combined = lax.optimization_barrier(jnp.sum(route_weights[..., None] * picked.astype(jnp.float32), axis=1))
    return combined.astype(jnp.bfloat16)

def reference(query_maps, key_maps, value_rows, head_lambda, head_gain, out_weight, expert_rows, expert_gain, routes, route_weights, gate_weight, up_weight, down_weight):
    mixed = mixer_half(query_maps, key_maps, value_rows, head_lambda, head_gain, out_weight)
    expert_out = expert_half(expert_rows, expert_gain, routes, route_weights, gate_weight, up_weight, down_weight)
    return (mixed, expert_out)
```

```python
import functools

import jax
import jax.numpy as jnp
from jax import lax
from jax.experimental import pallas as pl
from jax.experimental.pallas import tpu as pltpu
from jax.sharding import PartitionSpec as P

norm_eps = 1e-06
rope_base = 10000.0
log2e = 1.4426950408889634

NZ = 16
NX = 4
NY = 4
SLOTS = 12
PAIR = 2 * SLOTS
HALF = NZ // 2
ROWS = 256
COLS = 128

MESH = pl.DeviceIdType.MESH
bf16 = jnp.bfloat16
f32 = jnp.float32


def rope_turn(inputs, positions):
    half_dim = inputs.shape[-1] // 2
    inverse = rope_base ** (-2.0 * jnp.arange(half_dim, dtype=jnp.float32) / inputs.shape[-1])
    angles = positions.astype(jnp.float32)[:, None] * inverse[None, :]
    cos_table = jnp.cos(angles)[:, None, :]
    sin_table = jnp.sin(angles)[:, None, :]
    first_half = inputs[..., :half_dim]
    second_half = inputs[..., half_dim:]
    return jnp.concatenate(
        [
            first_half * cos_table - second_half * sin_table,
            second_half * cos_table + first_half * sin_table,
        ],
        axis=-1,
    )


def layer_kernel(
    q_t, kv_own, lam, gain, wout_hbm, disp, gate_hbm, up_hbm, down_hbm, pick0, pick1, rweights,
    mixed, expert_out,
    kv, acc, run_max, run_sum, wout, gate_w, up_w, down_w,
    exch_in, z_send, z_in, ag_a, ag_b, rs_a, rs_b, rs_a_in, rs_b_in, mid_a, mid_b, fin_a, fin_b,
    ret_send, ret, at_a, at_b, at_a_in, at_b_in, atm_a, atm_b, atf_a, atf_b,
    kv_recv, plus_send, minus_send, d2d_plus, d2d_minus, pair_send, pair_recv,
    z_sends, z_recvs, ret_sends, ret_recvs, plane_send, plane_recv, local_sem,
):
    ep = lax.axis_index("ep")
    tp = lax.axis_index("tp")
    z = ep // 2
    c = ep % 2
    y = tp // NX
    x = tp % NX
    partner = (z * 2 + 1 - c, tp)
    right = (((z + 1) % NZ) * 2 + c, tp)
    left = (((z + NZ - 1) % NZ) * 2 + c, tp)

    def z_peer(d):
        return (((z + d) % NZ) * 2 + c, tp)

    def x_peer(d):
        return (ep, y * NX + (x + d) % NX)

    def y_peer(d):
        return (ep, ((y + d) % NY) * NX + x)

    def remote(src, dst, send, recv, device):
        return pltpu.make_async_remote_copy(
            src_ref=src, dst_ref=dst, send_sem=send, recv_sem=recv,
            device_id=device, device_id_type=MESH,
        )

    loads = [
        pltpu.make_async_copy(gate_hbm, gate_w, local_sem.at[0]),
        pltpu.make_async_copy(up_hbm, up_w, local_sem.at[1]),
        pltpu.make_async_copy(down_hbm, down_w, local_sem.at[2]),
        pltpu.make_async_copy(wout_hbm, wout, local_sem.at[3]),
    ]

    barrier = pltpu.get_barrier_semaphore()
    for d in range(1, NZ):
        pl.semaphore_signal(barrier, inc=1, device_id=z_peer(d), device_id_type=MESH)
    pl.semaphore_signal(barrier, inc=1, device_id=partner, device_id_type=MESH)
    for d in range(1, 4):
        pl.semaphore_signal(barrier, inc=1, device_id=x_peer(d), device_id_type=MESH)
        pl.semaphore_signal(barrier, inc=1, device_id=y_peer(d), device_id_type=MESH)
    for load in loads:
        load.start()
    pl.semaphore_wait(barrier, NZ - 1 + 1 + 6)

    exch = remote(disp.at[1 - c], exch_in, pair_send.at[0], pair_recv.at[0], partner)
    exch.start()

    def kv_wait(slot, p):
        remote(
            kv.at[slot, p], kv.at[slot, p], plus_send.at[0, p], kv_recv.at[slot, p], left
        ).wait_recv()

    def kv_copy(src, slot, p, send, device):
        return remote(src, kv.at[slot, p], send, kv_recv.at[slot, p], device)

    exch.wait_recv()
    z_send[...] = (disp[c].astype(f32) + exch_in[...].astype(f32)).astype(bf16)
    z_in[z] = z_send[z]
    for d in range(1, NZ):
        remote(
            z_send.at[(z + d) % NZ], z_in.at[z], z_sends.at[d], z_recvs.at[d], z_peer(d)
        ).start()

    for p in range(2):
        @pl.when(z < NZ - 1)
        def _():
            kv_copy(kv_own.at[p], ep, p, plus_send.at[0, p], right).start()

        @pl.when(z <= 6 + p)
        def _():
            kv_copy(kv_own.at[p], ep, p, minus_send.at[0, p], left).start()

        @pl.when(c == 0)
        def _():
            kv_copy(kv_own.at[p], ep, p, d2d_plus.at[0, p], partner).start()

    scale = (128 ** -0.5) * log2e

    def fold(k_of, v_of, count, masked, first):
        for m in range(2):
            q_m = q_t[m * 128:(m + 1) * 128, :]
            scores = []
            for i in range(count):
                s = jnp.dot(k_of(i)[:, m * 128:(m + 1) * 128], q_m, preferred_element_type=f32)
                if masked:
                    rows = lax.broadcasted_iota(jnp.int32, s.shape, 0)
                    cols = lax.broadcasted_iota(jnp.int32, s.shape, 1)
                    s = jnp.where(rows <= cols, s, -1e30)
                scores.append(s)
            top = jnp.max(scores[0], axis=0, keepdims=True)
            for s in scores[1:]:
                top = jnp.maximum(top, jnp.max(s, axis=0, keepdims=True))
            top = top * scale
            if first:
                new_max = top
            else:
                old = run_max[m]
                new_max = jnp.maximum(old, top)
                alpha = jnp.exp2(old - new_max)
            total = None
            out = None
            for i in range(count):
                e = jnp.exp2(scores[i] * scale - new_max)
                t = jnp.sum(e, axis=0, keepdims=True)
                total = t if total is None else total + t
                o = jnp.dot(v_of(i), e.astype(bf16), preferred_element_type=f32)
                out = o if out is None else out + o
            run_max[m] = new_max
            if first:
                run_sum[m] = total
                acc[m] = out
            else:
                run_sum[m] = run_sum[m] * alpha + total
                acc[m] = acc[m] * alpha + out

    fold(lambda i: kv_own[0], lambda i: kv_own[1], 1, True, True)

    @pl.when(c == 1)
    def _():
        kv_wait(ep - 1, 0)
        kv_wait(ep - 1, 1)
        fold(lambda i: kv[ep - 1, 0], lambda i: kv[ep - 1, 1], 1, False, False)

    def fold_chip(chip):
        other = chip * 2 + 1 - c
        kv_wait(other, 0)
        kv_wait(other, 1)
        fold(
            lambda i: kv[chip * 2 + i, 0], lambda i: kv[chip * 2 + i, 1], 2, False, False
        )

    def plane_copies(index, half, src_of, dst_of, peer):
        return [
            remote(
                src_of(d), dst_of(d), plane_send.at[index, half, d - 1],
                plane_recv.at[index, half, d - 1], peer(d),
            )
            for d in range(1, 4)
        ]

    def start_all(copies):
        for cp in copies:
            cp.start()

    def wait_recvs(copies):
        for cp in copies:
            cp.wait_recv()

    def wait_sends(copies):
        for cp in copies:
            cp.wait_send()

    ag1_a = plane_copies(0, 0, lambda d: z_in.at[pl.ds(0, HALF)], lambda d: ag_a.at[y, x], x_peer)
    ag1_b = plane_copies(0, 1, lambda d: z_in.at[pl.ds(HALF, HALF)], lambda d: ag_b.at[x, y], y_peer)
    ag2_a = plane_copies(1, 0, lambda d: ag_a.at[y], lambda d: ag_a.at[y], y_peer)
    ag2_b = plane_copies(1, 1, lambda d: ag_b.at[x], lambda d: ag_b.at[x], x_peer)
    rs1_a = plane_copies(2, 0, lambda d: rs_a.at[(y + d) % NY], lambda d: rs_a_in.at[d - 1], y_peer)
    rs1_b = plane_copies(2, 1, lambda d: rs_b.at[(x + d) % NX], lambda d: rs_b_in.at[d - 1], x_peer)
    rs2_a = plane_copies(3, 0, lambda d: mid_a.at[(x + d) % NX], lambda d: fin_a.at[d - 1], x_peer)
    rs2_b = plane_copies(3, 1, lambda d: mid_b.at[(y + d) % NY], lambda d: fin_b.at[d - 1], y_peer)
    at1_a = plane_copies(4, 0, lambda d: at_a.at[(y + d) % NY], lambda d: at_a_in.at[d - 1], y_peer)
    at1_b = plane_copies(4, 1, lambda d: at_b.at[(x + d) % NX], lambda d: at_b_in.at[d - 1], x_peer)
    at2_a = plane_copies(5, 0, lambda d: atm_a.at[(x + d) % NX], lambda d: atf_a.at[d - 1], x_peer)
    at2_b = plane_copies(5, 1, lambda d: atm_b.at[(y + d) % NY], lambda d: atf_b.at[d - 1], y_peer)

    def gather_one():
        for d in range(1, NZ):
            remote(
                z_send.at[d], z_in.at[(z + NZ - d) % NZ], z_sends.at[d], z_recvs.at[d], z_peer(d)
            ).wait_recv()
        ag_a[y, x] = z_in[0:HALF]
        ag_b[x, y] = z_in[HALF:NZ]
        start_all(ag1_a)
        start_all(ag1_b)

    def gather_two():
        for d in range(1, 4):
            remote(
                ag_a.at[y, x], ag_a.at[y, (x + 4 - d) % NX], plane_send.at[0, 0, d - 1],
                plane_recv.at[0, 0, d - 1], x_peer(d),
            ).wait_recv()
            remote(
                ag_b.at[x, y], ag_b.at[x, (y + 4 - d) % NY], plane_send.at[0, 1, d - 1],
                plane_recv.at[0, 1, d - 1], y_peer(d),
            ).wait_recv()
        start_all(ag2_a)
        start_all(ag2_b)

    def expert(half):
        if half == 0:
            for load in loads[:3]:
                load.wait()
        for d in range(1, 4):
            if half == 0:
                remote(
                    ag_a.at[y], ag_a.at[(y + 4 - d) % NY], plane_send.at[1, 0, d - 1],
                    plane_recv.at[1, 0, d - 1], y_peer(d),
                ).wait_recv()
            else:
                remote(
                    ag_b.at[x], ag_b.at[(x + 4 - d) % NX], plane_send.at[1, 1, d - 1],
                    plane_recv.at[1, 1, d - 1], x_peer(d),
                ).wait_recv()
        n = HALF * PAIR
        pieces = [
            (ag_a[i, j] if half == 0 else ag_b[j, i]).reshape(n, COLS)
            for i in range(NY)
            for j in range(NX)
        ]
        rows = jnp.concatenate(pieces, axis=1)
        g = jnp.dot(rows, gate_w[...], preferred_element_type=f32)
        u = jnp.dot(rows, up_w[...], preferred_element_type=f32)
        hidden = (g / (1.0 + jnp.exp(-g)) * u).astype(bf16)
        for i in range(NY):
            for j in range(NX):
                at = (i * NX + j) * COLS
                part = jnp.dot(
                    hidden, down_w[:, at:at + COLS], preferred_element_type=f32
                ).astype(bf16)
                if half == 0:
                    rs_a[i, j] = part
                else:
                    rs_b[j, i] = part
        start_all(rs1_a if half == 0 else rs1_b)

    def sum_one():
        wait_recvs(rs1_a)
        for j in range(4):
            t = rs_a[y, j].astype(f32)
            for d in range(3):
                t = t + rs_a_in[d, j].astype(f32)
            mid_a[j] = t.astype(bf16)
        start_all(rs2_a)
        wait_recvs(rs1_b)
        for j in range(4):
            t = rs_b[x, j].astype(f32)
            for d in range(3):
                t = t + rs_b_in[d, j].astype(f32)
            mid_b[j] = t.astype(bf16)
        start_all(rs2_b)

    def sum_two():
        wait_recvs(rs2_a)
        wait_recvs(rs2_b)
        t = mid_a[x].astype(f32)
        for d in range(3):
            t = t + fin_a[d].astype(f32)
        ret_send[0:HALF] = t.astype(bf16).reshape(HALF, PAIR, COLS)
        t = mid_b[y].astype(f32)
        for d in range(3):
            t = t + fin_b[d].astype(f32)
        ret_send[HALF:NZ] = t.astype(bf16).reshape(HALF, PAIR, COLS)
        ret[0, z] = ret_send[z]
        for d in range(1, NZ):
            remote(
                ret_send.at[(z + d) % NZ], ret.at[0, z], ret_sends.at[d], ret_recvs.at[d],
                z_peer(d),
            ).start()

    def tick(s, carry):
        zl = jnp.maximum(z - s, 0)
        zr = (z + s) % NZ
        wrapped = z + s >= NZ

        def plus(p, last):
            @pl.when((s <= last) & (s <= z))
            def _():
                slot = zl * 2 + c
                kv_wait(slot, p)

                @pl.when((z < NZ - 1) & (s < last))
                def _():
                    kv_copy(kv.at[slot, p], slot, p, plus_send.at[s, p], right).start()

                kv_copy(kv.at[slot, p], slot, p, d2d_plus.at[s, p], partner).start()

        def minus(p, last):
            @pl.when((s <= last) & (zr <= 6 + p))
            def _():
                slot = zr * 2 + c
                kv_wait(slot, p)

                @pl.when(s < last)
                def _():
                    kv_copy(kv.at[slot, p], slot, p, minus_send.at[s, p], left).start()

                @pl.when(wrapped)
                def _():
                    kv_copy(kv.at[slot, p], slot, p, d2d_minus.at[s, p], partner).start()

        plus(0, 8)
        minus(0, 7)

        @pl.when(s == 2)
        def _():
            gather_one()

        @pl.when(s == 3)
        def _():
            gather_two()

        @pl.when((s >= 2) & (s - 1 <= z))
        def _():
            fold_chip(jnp.maximum(z - s + 1, 0))

        plus(1, 7)
        minus(1, 8)

        @pl.when(s == 5)
        def _():
            expert(0)

        @pl.when(s == 6)
        def _():
            expert(1)

        @pl.when(s == 7)
        def _():
            sum_one()

        @pl.when(s == 8)
        def _():
            sum_two()

        @pl.when((s >= 2) & (s - 1 <= 7) & (z + s - 1 >= NZ))
        def _():
            fold_chip(jnp.maximum(z + s - 1 - NZ, 0))

        return carry

    lax.fori_loop(1, 10, tick, 0)

    first = acc[0] / run_sum[0]
    second = acc[1] / run_sum[1]
    diff = first - lam[0, 0] * second
    mean = jnp.mean(diff * diff, axis=0, keepdims=True)
    head_t = diff * lax.rsqrt(mean + norm_eps) * gain[...]
    head = head_t.T.astype(bf16)
    loads[3].wait()
    for i in range(NY):
        for j in range(NX):
            at = (i * NX + j) * COLS
            part = jnp.dot(head, wout[:, at:at + COLS], preferred_element_type=f32).astype(bf16)
            at_a[i, j] = part[:ROWS // 2]
            at_b[j, i] = part[ROWS // 2:]
    start_all(at1_a)
    start_all(at1_b)

    for d in range(1, NZ):
        remote(
            ret_send.at[d], ret.at[0, (z + NZ - d) % NZ], ret_sends.at[d], ret_recvs.at[d],
            z_peer(d),
        ).wait_recv()
    back = remote(ret.at[0], ret.at[1], pair_send.at[1], pair_recv.at[1], partner)
    back.start()

    wait_recvs(at1_a)
    for j in range(4):
        t = at_a[y, j].astype(f32)
        for d in range(3):
            t = t + at_a_in[d, j].astype(f32)
        atm_a[j] = t.astype(bf16)
    start_all(at2_a)
    wait_recvs(at1_b)
    for j in range(4):
        t = at_b[x, j].astype(f32)
        for d in range(3):
            t = t + at_b_in[d, j].astype(f32)
        atm_b[j] = t.astype(bf16)
    start_all(at2_b)

    back.wait_recv()
    rows = ret[...].reshape(2 * NZ * PAIR, COLS)
    chosen = jnp.dot(pick0[...], rows, preferred_element_type=f32) * rweights[:, 0:1]
    chosen = chosen + jnp.dot(pick1[...], rows, preferred_element_type=f32) * rweights[:, 1:2]
    expert_out[...] = chosen.astype(bf16)

    wait_recvs(at2_a)
    t = atm_a[x].astype(f32)
    for d in range(3):
        t = t + atf_a[d].astype(f32)
    mixed[0:ROWS // 2] = t.astype(bf16)
    wait_recvs(at2_b)
    t = atm_b[y].astype(f32)
    for d in range(3):
        t = t + atf_b[d].astype(f32)
    mixed[ROWS // 2:ROWS] = t.astype(bf16)

    exch.wait_send()
    back.wait_send()
    for d in range(1, NZ):
        remote(
            z_send.at[d], z_in.at[d], z_sends.at[d], z_recvs.at[d], z_peer(d)
        ).wait_send()
        remote(
            ret_send.at[d], ret.at[0, d], ret_sends.at[d], ret_recvs.at[d], z_peer(d)
        ).wait_send()
    for copies in (
        ag1_a, ag1_b, ag2_a, ag2_b, rs1_a, rs1_b, rs2_a, rs2_b, at1_a, at1_b, at2_a, at2_b
    ):
        wait_sends(copies)

    def sent(sem, p):
        remote(kv_own.at[p], kv.at[0, p], sem, kv_recv.at[0, p], left).wait_send()

    for p in range(2):
        @pl.when(z < NZ - 1)
        def _():
            sent(plus_send.at[0, p], p)

        @pl.when(z <= 6 + p)
        def _():
            sent(minus_send.at[0, p], p)

        @pl.when(c == 0)
        def _():
            sent(d2d_plus.at[0, p], p)

    def drain(s, carry):
        zr = (z + s) % NZ
        for p in range(2):
            last_p, last_m = 8 - p, 7 + p

            @pl.when((s <= last_p) & (s <= z))
            def _():
                @pl.when((z < NZ - 1) & (s < last_p))
                def _():
                    sent(plus_send.at[s, p], p)

                sent(d2d_plus.at[s, p], p)

            @pl.when((s <= last_m) & (zr <= 6 + p))
            def _():
                @pl.when(s < last_m)
                def _():
                    sent(minus_send.at[s, p], p)

                @pl.when(z + s >= NZ)
                def _():
                    sent(d2d_minus.at[s, p], p)

        return carry

    lax.fori_loop(1, 9, drain, 0)


def call_kernel(*operands):
    vmem = pl.BlockSpec(memory_space=pltpu.VMEM)
    hbm = pl.BlockSpec(memory_space=pl.ANY)
    smem = pl.BlockSpec(memory_space=pltpu.SMEM)
    n = HALF * PAIR
    h = ROWS // 2
    V = lambda *shape: pltpu.VMEM(shape, bf16)
    D = lambda *shape: pltpu.SemaphoreType.DMA(shape)
    return pl.pallas_call(
        layer_kernel,
        out_shape=(
            jax.ShapeDtypeStruct((ROWS, COLS), bf16),
            jax.ShapeDtypeStruct((128, COLS), bf16),
        ),
        in_specs=[vmem, vmem, smem, vmem, hbm, vmem, hbm, hbm, hbm, vmem, vmem, vmem],
        out_specs=(vmem, vmem),
        scratch_shapes=[
            V(2 * NZ, 2, ROWS, ROWS),
            pltpu.VMEM((2, ROWS, ROWS), f32),
            pltpu.VMEM((2, 1, ROWS), f32),
            pltpu.VMEM((2, 1, ROWS), f32),
            V(ROWS, 2048), V(2048, 256), V(2048, 256), V(256, 2048),
            V(NZ, PAIR, COLS), V(NZ, PAIR, COLS), V(NZ, PAIR, COLS),
            V(4, 4, HALF, PAIR, COLS), V(4, 4, HALF, PAIR, COLS),
            V(4, 4, n, COLS), V(4, 4, n, COLS), V(3, 4, n, COLS), V(3, 4, n, COLS),
            V(4, n, COLS), V(4, n, COLS), V(3, n, COLS), V(3, n, COLS),
            V(NZ, PAIR, COLS), V(2, NZ, PAIR, COLS),
            V(4, 4, h, COLS), V(4, 4, h, COLS), V(3, 4, h, COLS), V(3, 4, h, COLS),
            V(4, h, COLS), V(4, h, COLS), V(3, h, COLS), V(3, h, COLS),
            D(32, 2), D(8, 2), D(8, 2), D(9, 2), D(9, 2), D(2), D(2),
            D(NZ), D(NZ), D(NZ), D(NZ), D(6, 2, 3), D(6, 2, 3), D(4),
        ],
        compiler_params=pltpu.CompilerParams(
            collective_id=0, has_side_effects=True, vmem_limit_bytes=60 * 1024 * 1024
        ),
    )(*operands)


def on_device(
    query_maps, key_maps, value_rows, head_lambda, head_gain, out_weight,
    expert_rows, expert_gain, routes, route_weights, gate_weight, up_weight, down_weight,
):
    ep = lax.axis_index("ep")
    tp = lax.axis_index("tp")
    core = ep % 2
    row_count = query_maps.shape[0]
    positions = ep * row_count + jnp.arange(row_count, dtype=jnp.int32)

    def turned(maps):
        wide = maps.astype(f32).reshape(row_count, 2, 128)
        return rope_turn(wide, positions).astype(bf16).reshape(row_count, 256)

    q_t = turned(query_maps).T
    kv_own = jnp.stack([turned(key_maps), value_rows.T])

    inputs = expert_rows.astype(f32)
    normed = (
        inputs
        * lax.rsqrt(jnp.mean(inputs * inputs, axis=-1, keepdims=True) + norm_eps)
        * expert_gain
    ).astype(bf16)
    mine = lax.dynamic_slice_in_dim(normed, tp * COLS, COLS, 1)
    tokens, picks = routes.shape
    ids = routes.reshape(-1)
    one_hot = (ids[:, None] == jnp.arange(32, dtype=jnp.int32)[None, :]).astype(f32)
    order = jnp.arange(tokens * picks, dtype=jnp.int32)
    before = (order[None, :] < order[:, None]).astype(bf16)
    counts = jnp.dot(before, one_hot.astype(bf16), preferred_element_type=f32)
    slot = jnp.sum(counts * one_hot, axis=1).astype(jnp.int32).reshape(tokens, picks)
    base = (routes // 2) * PAIR + core * SLOTS + slot
    to_row = (routes % 2) * (NZ * PAIR) + base
    from_row = (routes % 2 != core).astype(jnp.int32) * (NZ * PAIR) + base
    lines = jnp.arange(2 * NZ * PAIR, dtype=jnp.int32)
    place = (lines[:, None] == to_row[None, :, 0]) | (lines[:, None] == to_row[None, :, 1])
    disp = jnp.dot(place.astype(bf16), mine, preferred_element_type=f32).astype(bf16)
    disp = disp.reshape(2, NZ, PAIR, COLS)
    pick0 = (from_row[:, 0:1] == lines[None, :]).astype(bf16)
    pick1 = (from_row[:, 1:2] == lines[None, :]).astype(bf16)

    return call_kernel(
        q_t, kv_own, head_lambda.reshape(1, 1), head_gain.reshape(-1, 1), out_weight,
        disp, gate_weight[0], up_weight[0], down_weight[0], pick0, pick1, route_weights,
    )


def solution(mesh):
    placed = (
        P("ep", "tp"),
        P("ep", "tp"),
        P("ep", "tp"),
        P("tp"),
        P(),
        P("tp", None),
        P("ep", None),
        P(),
        P("ep", None),
        P("ep", None),
        P("ep", None, "tp"),
        P("ep", None, "tp"),
        P("ep", "tp", None),
    )
    return jax.shard_map(
        on_device,
        mesh=mesh,
        in_specs=placed,
        out_specs=(P("ep", "tp"), P("ep", "tp")),
        check_vma=False,
    )
```

```python
import functools

import jax
import jax.numpy as jnp
from jax import lax
from jax.experimental import pallas as pl
from jax.experimental.pallas import tpu as pltpu
from jax.sharding import PartitionSpec as P

norm_eps = 1e-06
rope_base = 10000.0
log2e = 1.4426950408889634

NZ = 16
NX = 4
NY = 4
SLOTS = 12
PAIR = 2 * SLOTS
HALF = NZ // 2
ROWS = 256
COLS = 128

MESH = pl.DeviceIdType.MESH
bf16 = jnp.bfloat16
f32 = jnp.float32


def layer_kernel(
    q_hbm, k_hbm, v_hbm, cos_hbm, sin_hbm, lam, gain_hbm, wout_hbm, rows_hbm, rgain_hbm,
    routes_hbm, rweights_hbm, gate_hbm, up_hbm, down_hbm,
    mixed_hbm, expert_hbm,
    q_in, k_in, v_in, cos_t, sin_t, gain, row_in, rgain, routes, rweights,
    q_t, kv_own, disp, pick, spread, mixed, expert_out,
    kv, acc, run_max, run_sum, wout, gate_w, up_w, down_w,
    exch_in, z_send, z_in, ag_a, ag_b, rs_a, rs_b, rs_a_in, rs_b_in, mid_a, mid_b, fin_a, fin_b,
    ret_send, ret, at_a, at_b, at_a_in, at_b_in, atm_a, atm_b, atf_a, atf_b,
    ring_recv, core_recv, kv_sent, pair_send, pair_recv,
    z_sent, z_came, ret_sent, ret_came, plane_send, plane_recv, local_sem,
):
    ep = lax.axis_index("ep")
    tp = lax.axis_index("tp")
    z = ep // 2
    c = ep % 2
    y = tp // NX
    x = tp % NX
    partner = (z * 2 + 1 - c, tp)
    right = (((z + 1) % NZ) * 2 + c, tp)
    left = (((z + NZ - 1) % NZ) * 2 + c, tp)

    def z_peer(d):
        return (((z + d) % NZ) * 2 + c, tp)

    def x_peer(d):
        return (ep, y * NX + (x + d) % NX)

    def y_peer(d):
        return (ep, ((y + d) % NY) * NX + x)

    def remote(src, dst, send, recv, device):
        return pltpu.make_async_remote_copy(
            src_ref=src, dst_ref=dst, send_sem=send, recv_sem=recv,
            device_id=device, device_id_type=MESH,
        )

    loads = [
        pltpu.make_async_copy(src, dst, local_sem.at[i])
        for i, (src, dst) in enumerate(
            (
                (k_hbm, k_in), (cos_hbm, cos_t), (sin_hbm, sin_t), (v_hbm, v_in),
                (rows_hbm, row_in), (routes_hbm, routes), (rgain_hbm, rgain), (q_hbm, q_in),
                (rweights_hbm, rweights), (gate_hbm, gate_w), (up_hbm, up_w),
                (down_hbm, down_w), (wout_hbm, wout), (gain_hbm, gain),
            )
        )
    ]

    barrier = pltpu.get_barrier_semaphore()
    for d in range(NZ // 2, 0, -1):
        pl.semaphore_signal(barrier, inc=1, device_id=z_peer(d), device_id_type=MESH)
        if d < NZ // 2:
            pl.semaphore_signal(barrier, inc=1, device_id=z_peer(NZ - d), device_id_type=MESH)
    for d in range(1, 4):
        pl.semaphore_signal(barrier, inc=1, device_id=x_peer(d), device_id_type=MESH)
        pl.semaphore_signal(barrier, inc=1, device_id=y_peer(d), device_id_type=MESH)
    pl.semaphore_signal(barrier, inc=1, device_id=partner, device_id_type=MESH)
    for load in loads:
        load.start()

    def turned(maps, m):
        wide = maps[:, m * 128:(m + 1) * 128].astype(f32)
        return wide * cos_t[...] + pltpu.roll(wide, 64, 1) * sin_t[...]

    for i in range(3):
        loads[i].wait()
    for m in range(2):
        kv_own[0, :, m * 128:(m + 1) * 128] = turned(k_in, m).astype(bf16)
    loads[3].wait()
    kv_own[1] = v_in[...].astype(f32).T.astype(bf16)

    for i in range(4, 7):
        loads[i].wait()
    wide = row_in[...].astype(f32)
    level = lax.rsqrt(jnp.mean(wide * wide, axis=1, keepdims=True) + norm_eps)
    column = pl.ds(pl.multiple_of(tp * COLS, COLS), COLS)
    normed = (row_in[:, column].astype(f32) * level * rgain[:, column]).astype(bf16)
    chosen = [routes[k:k + 1, :] for k in range(2)]
    names = lax.broadcasted_iota(jnp.int32, (32, 128), 0)
    hot = [(names == r).astype(f32) for r in chosen]
    earlier = (
        lax.broadcasted_iota(jnp.int32, (128, 128), 0)
        < lax.broadcasted_iota(jnp.int32, (128, 128), 1)
    )
    counts = jnp.dot(
        (hot[0] + hot[1]).astype(bf16), earlier.astype(f32).astype(bf16),
        preferred_element_type=f32,
    )
    lines = lax.broadcasted_iota(jnp.int32, (2 * NZ * PAIR, 128), 0).astype(f32)
    base = [
        ((r // 2) * PAIR + c * SLOTS).astype(f32) + jnp.sum(counts * h, axis=0, keepdims=True)
        for r, h in zip(chosen, hot)
    ]
    block = float(NZ * PAIR)
    to_row = [b + (r % 2).astype(f32) * block for b, r in zip(base, chosen)]
    from_row = [
        b + jnp.where(r % 2 == c, 0.0, block) for b, r in zip(base, chosen)
    ]
    place = jnp.where((lines == to_row[0]) | (lines == to_row[1]), 1.0, 0.0).astype(bf16)
    disp[...] = (
        jnp.dot(place, normed, preferred_element_type=f32)
        .astype(bf16)
        .reshape(2, NZ, PAIR, COLS)
    )
    pl.semaphore_wait(barrier, NZ - 1 + 1 + 6)

    exch = remote(disp.at[1 - c], exch_in, pair_send.at[0], pair_recv.at[0], partner)
    exch.start()

    def ring_piece(chip, p):
        return kv.at[chip * 4 + c * 2 + p]

    def ring_wait(chip, p):
        here = ring_piece(chip, p)
        remote(here, here, kv_sent.at[0], ring_recv.at[chip, p], left).wait_recv()

    def core_wait(chip):
        here = kv.at[pl.ds(chip * 4 + 2 - c * 2, 2)]
        remote(here, here, kv_sent.at[2], core_recv.at[chip], partner).wait_recv()

    def ring_copy(src, chip, p, way, device):
        return remote(src, ring_piece(chip, p), kv_sent.at[way], ring_recv.at[chip, p], device)

    def core_copy(src, chip, p):
        return remote(src, ring_piece(chip, p), kv_sent.at[2], core_recv.at[chip], partner)

    def send_own(p):
        @pl.when(z < NZ - 1)
        def _():
            ring_copy(kv_own.at[p], z, p, 0, right).start()

        @pl.when(z <= 6 + p)
        def _():
            ring_copy(kv_own.at[p], z, p, 1, left).start()

        @pl.when(c == 0)
        def _():
            core_copy(kv_own.at[p], z, p).start()

    send_own(0)
    exch.wait_recv()
    z_send[...] = (disp[c].astype(f32) + exch_in[...].astype(f32)).astype(bf16)
    z_in[z] = z_send[z]
    for d in range(1, NZ):
        remote(
            z_send.at[(z + d) % NZ], z_in.at[z], z_sent.at[0], z_came.at[0], z_peer(d)
        ).start()
    send_own(1)

    loads[7].wait()
    for m in range(2):
        q_t[m * 128:(m + 1) * 128, :] = turned(q_in, m).T.astype(bf16)
    loads[8].wait()
    for k in range(2):
        pick[k] = jnp.where(lines == from_row[k], 1.0, 0.0).T.astype(bf16)
        spread[k] = jnp.broadcast_to(rweights[k:k + 1, :], (128, 128)).T

    scale = (128 ** -0.5) * log2e

    def fold(k_of, v_of, count, masked, first):
        for m in range(2):
            q_m = q_t[m * 128:(m + 1) * 128, :]
            scores = []
            for i in range(count):
                s = jnp.dot(k_of(i)[:, m * 128:(m + 1) * 128], q_m, preferred_element_type=f32)
                if masked:
                    rows = lax.broadcasted_iota(jnp.int32, s.shape, 0)
                    cols = lax.broadcasted_iota(jnp.int32, s.shape, 1)
                    s = jnp.where(rows <= cols, s, -1e30)
                scores.append(s)
            top = jnp.max(scores[0], axis=0, keepdims=True)
            for s in scores[1:]:
                top = jnp.maximum(top, jnp.max(s, axis=0, keepdims=True))
            top = top * scale
            if first:
                new_max = top
            else:
                old = run_max[m]
                new_max = jnp.maximum(old, top)
                alpha = jnp.exp2(old - new_max)
            total = None
            out = None
            for i in range(count):
                e = jnp.exp2(scores[i] * scale - new_max)
                t = jnp.sum(e, axis=0, keepdims=True)
                total = t if total is None else total + t
                o = jnp.dot(v_of(i), e.astype(bf16), preferred_element_type=f32)
                out = o if out is None else out + o
            run_max[m] = new_max
            if first:
                run_sum[m] = total
                acc[m] = out
            else:
                run_sum[m] = run_sum[m] * alpha + total
                acc[m] = acc[m] * alpha + out

    fold(lambda i: kv_own[0], lambda i: kv_own[1], 1, True, True)

    @pl.when(c == 1)
    def _():
        core_wait(z)
        fold(lambda i: kv[z * 4], lambda i: kv[z * 4 + 1], 1, False, False)

    def fold_chip(chip):
        core_wait(chip)
        fold(
            lambda i: kv[chip * 4 + i * 2], lambda i: kv[chip * 4 + i * 2 + 1], 2, False, False
        )

    def plane_copies(index, half, src_of, dst_of, peer):
        return [
            remote(
                src_of(d), dst_of(d), plane_send.at[index, half],
                plane_recv.at[index, half], peer(d),
            )
            for d in range(1, 4)
        ]

    def start_all(copies):
        for cp in copies:
            cp.start()

    def three(index, half, ref):
        return remote(
            ref, ref, plane_send.at[index, half], plane_recv.at[index, half], partner
        )

    ag1_a = plane_copies(0, 0, lambda d: z_in.at[pl.ds(0, HALF)], lambda d: ag_a.at[y, x], x_peer)
    ag1_b = plane_copies(0, 1, lambda d: z_in.at[pl.ds(HALF, HALF)], lambda d: ag_b.at[x, y], y_peer)
    ag2_a = plane_copies(1, 0, lambda d: ag_a.at[y], lambda d: ag_a.at[y], y_peer)
    ag2_b = plane_copies(1, 1, lambda d: ag_b.at[x], lambda d: ag_b.at[x], x_peer)
    rs1_a = plane_copies(2, 0, lambda d: rs_a.at[(y + d) % NY], lambda d: rs_a_in.at[d - 1], y_peer)
    rs1_b = plane_copies(2, 1, lambda d: rs_b.at[(x + d) % NX], lambda d: rs_b_in.at[d - 1], x_peer)
    rs2_a = plane_copies(3, 0, lambda d: mid_a.at[(x + d) % NX], lambda d: fin_a.at[d - 1], x_peer)
    rs2_b = plane_copies(3, 1, lambda d: mid_b.at[(y + d) % NY], lambda d: fin_b.at[d - 1], y_peer)
    at1_a = plane_copies(4, 0, lambda d: at_a.at[(y + d) % NY], lambda d: at_a_in.at[d - 1], y_peer)
    at1_b = plane_copies(4, 1, lambda d: at_b.at[(x + d) % NX], lambda d: at_b_in.at[d - 1], x_peer)
    at2_a = plane_copies(5, 0, lambda d: atm_a.at[(x + d) % NX], lambda d: atf_a.at[d - 1], x_peer)
    at2_b = plane_copies(5, 1, lambda d: atm_b.at[(y + d) % NY], lambda d: atf_b.at[d - 1], y_peer)

    def gather_one():
        most = pl.ds(0, NZ - 1)
        remote(
            z_send.at[most], z_in.at[most], z_sent.at[0], z_came.at[0], partner
        ).wait_recv()
        ag_a[y, x] = z_in[0:HALF]
        ag_b[x, y] = z_in[HALF:NZ]
        start_all(ag1_a)
        start_all(ag1_b)

    def gather_two():
        three(0, 0, ag_a.at[0, pl.ds(0, 3)]).wait_recv()
        three(0, 1, ag_b.at[0, pl.ds(0, 3)]).wait_recv()
        start_all(ag2_a)
        start_all(ag2_b)

    def expert(half):
        if half == 0:
            for load in loads[9:12]:
                load.wait()
        three(1, half, (ag_b if half else ag_a).at[pl.ds(0, 3)]).wait_recv()
        n = HALF * PAIR
        pieces = [
            (ag_a[i, j] if half == 0 else ag_b[j, i]).reshape(n, COLS)
            for i in range(NY)
            for j in range(NX)
        ]
        rows = jnp.concatenate(pieces, axis=1)
        g = jnp.dot(rows, gate_w[...], preferred_element_type=f32)
        u = jnp.dot(rows, up_w[...], preferred_element_type=f32)
        hidden = (g / (1.0 + jnp.exp(-g)) * u).astype(bf16)
        for i in range(NY):
            for j in range(NX):
                at = (i * NX + j) * COLS
                part = jnp.dot(
                    hidden, down_w[:, at:at + COLS], preferred_element_type=f32
                ).astype(bf16)
                if half == 0:
                    rs_a[i, j] = part
                else:
                    rs_b[j, i] = part
        start_all(rs1_a if half == 0 else rs1_b)

    def sum_one_a():
        three(2, 0, rs_a_in).wait_recv()
        for j in range(4):
            t = rs_a[y, j].astype(f32)
            for d in range(3):
                t = t + rs_a_in[d, j].astype(f32)
            mid_a[j] = t.astype(bf16)
        start_all(rs2_a)

    def sum_one_b():
        three(2, 1, rs_b_in).wait_recv()
        for j in range(4):
            t = rs_b[x, j].astype(f32)
            for d in range(3):
                t = t + rs_b_in[d, j].astype(f32)
            mid_b[j] = t.astype(bf16)
        start_all(rs2_b)

    def sum_two():
        three(3, 0, fin_a).wait_recv()
        three(3, 1, fin_b).wait_recv()
        t = mid_a[x].astype(f32)
        for d in range(3):
            t = t + fin_a[d].astype(f32)
        ret_send[0:HALF] = t.astype(bf16).reshape(HALF, PAIR, COLS)
        t = mid_b[y].astype(f32)
        for d in range(3):
            t = t + fin_b[d].astype(f32)
        ret_send[HALF:NZ] = t.astype(bf16).reshape(HALF, PAIR, COLS)
        ret[0, z] = ret_send[z]
        for d in range(1, NZ):
            remote(
                ret_send.at[(z + d) % NZ], ret.at[0, z], ret_sent.at[0], ret_came.at[0],
                z_peer(d),
            ).start()

    def tick(s, carry):
        zl = jnp.maximum(z - s, 0)
        zr = (z + s) % NZ
        wrapped = z + s >= NZ

        def plus(p, last):
            @pl.when((s <= last) & (s <= z))
            def _():
                ring_wait(zl, p)

                @pl.when((z < NZ - 1) & (s < last))
                def _():
                    ring_copy(ring_piece(zl, p), zl, p, 0, right).start()

                core_copy(ring_piece(zl, p), zl, p).start()

        def minus(p, last):
            @pl.when((s <= last) & (zr <= 6 + p))
            def _():
                ring_wait(zr, p)

                @pl.when(s < last)
                def _():
                    ring_copy(ring_piece(zr, p), zr, p, 1, left).start()

                @pl.when(wrapped)
                def _():
                    core_copy(ring_piece(zr, p), zr, p).start()

        def fold_minus():
            @pl.when((s >= 2) & (s - 1 <= 7) & (z + s - 1 >= NZ))
            def _():
                fold_chip(jnp.maximum(z + s - 1 - NZ, 0))

        plus(0, 8)
        minus(0, 7)

        @pl.when(s == 5)
        def _():
            expert(1)

        @pl.when(s == 7)
        def _():
            sum_one_a()

        @pl.when((s >= 2) & (s - 1 <= z))
        def _():
            fold_chip(jnp.maximum(z - s + 1, 0))

        @pl.when(s == 8)
        def _():
            fold_minus()

        plus(1, 7)
        minus(1, 8)

        @pl.when(s == 1)
        def _():
            gather_one()

        @pl.when(s == 2)
        def _():
            gather_two()

        @pl.when(s == 4)
        def _():
            expert(0)

        @pl.when(s == 7)
        def _():
            sum_one_b()

        @pl.when(s < 8)
        def _():
            fold_minus()

        return carry

    lax.fori_loop(1, 10, tick, 0)

    sum_two()

    first = acc[0] / run_sum[0]
    second = acc[1] / run_sum[1]
    diff = first - lam[0, 0] * second
    mean = jnp.mean(diff * diff, axis=0, keepdims=True)
    head_t = diff * lax.rsqrt(mean + norm_eps)
    for load in loads[12:14]:
        load.wait()
    head = (head_t.T * gain[...]).astype(bf16)
    for i in range(NY):
        for j in range(NX):
            at = (i * NX + j) * COLS
            part = jnp.dot(head, wout[:, at:at + COLS], preferred_element_type=f32).astype(bf16)
            at_a[i, j] = part[:ROWS // 2]
            at_b[j, i] = part[ROWS // 2:]
    start_all(at1_a)
    start_all(at1_b)

    three(4, 0, at_a_in).wait_recv()
    for j in range(4):
        t = at_a[y, j].astype(f32)
        for d in range(3):
            t = t + at_a_in[d, j].astype(f32)
        atm_a[j] = t.astype(bf16)
    start_all(at2_a)
    three(4, 1, at_b_in).wait_recv()
    for j in range(4):
        t = at_b[x, j].astype(f32)
        for d in range(3):
            t = t + at_b_in[d, j].astype(f32)
        atm_b[j] = t.astype(bf16)
    start_all(at2_b)

    most = pl.ds(0, NZ - 1)
    remote(
        ret_send.at[most], ret.at[0, most], ret_sent.at[0], ret_came.at[0], partner
    ).wait_recv()
    back = remote(ret.at[0], ret.at[1], pair_send.at[1], pair_recv.at[1], partner)
    back.start()

    back.wait_recv()
    rows = ret[...].reshape(2 * NZ * PAIR, COLS)
    mixture = jnp.dot(pick[0], rows, preferred_element_type=f32) * spread[0]
    mixture = mixture + jnp.dot(pick[1], rows, preferred_element_type=f32) * spread[1]
    expert_out[...] = mixture.astype(bf16)
    results = [
        pltpu.make_async_copy(expert_out, expert_hbm, local_sem.at[14]),
        pltpu.make_async_copy(mixed, mixed_hbm, local_sem.at[15]),
    ]
    results[0].start()

    three(5, 0, atf_a).wait_recv()
    t = atm_a[x].astype(f32)
    for d in range(3):
        t = t + atf_a[d].astype(f32)
    mixed[0:ROWS // 2] = t.astype(bf16)
    three(5, 1, atf_b).wait_recv()
    t = atm_b[y].astype(f32)
    for d in range(3):
        t = t + atf_b[d].astype(f32)
    mixed[ROWS // 2:ROWS] = t.astype(bf16)
    results[1].start()

    exch.wait_send()
    back.wait_send()
    remote(z_send.at[most], z_in.at[most], z_sent.at[0], z_came.at[0], partner).wait_send()
    remote(
        ret_send.at[most], ret.at[0, most], ret_sent.at[0], ret_came.at[0], partner
    ).wait_send()
    for half in range(2):
        three(0, half, ag_a.at[0, pl.ds(0, 3)]).wait_send()
        three(1, half, ag_a.at[pl.ds(0, 3)]).wait_send()
        three(2, half, rs_a_in).wait_send()
        three(3, half, fin_a).wait_send()
        three(4, half, at_a_in).wait_send()
        three(5, half, atf_a).wait_send()

    def sent(way, count):
        if count:
            here = kv.at[pl.ds(0, count)]
            remote(here, here, kv_sent.at[way], core_recv.at[0], partner).wait_send()

    for at in range(NZ):
        @pl.when(z == at)
        def _():
            came_plus = [min(at, 8 - p) for p in range(2)]
            on_plus = [0 if at == NZ - 1 else 1 + min(at, 7 - p) for p in range(2)]
            on_minus = [
                sum((at + s) % NZ <= 6 + p for s in range(7 + p)) for p in range(2)
            ]
            wrapped = [
                sum((at + s) % NZ <= 6 + p and at + s >= NZ for s in range(1, 8 + p))
                for p in range(2)
            ]
            sent(0, sum(on_plus))
            sent(1, sum(on_minus))
            passed = sum(came_plus) + sum(wrapped)

            @pl.when(c == 0)
            def _():
                sent(2, passed + 2)

            @pl.when(c == 1)
            def _():
                sent(2, passed)

    for result in results:
        result.wait()


def call_kernel(*operands):
    hbm = pl.BlockSpec(memory_space=pl.ANY)
    smem = pl.BlockSpec(memory_space=pltpu.SMEM)
    n = HALF * PAIR
    h = ROWS // 2
    V = lambda *shape: pltpu.VMEM(shape, bf16)
    F = lambda *shape: pltpu.VMEM(shape, f32)
    D = lambda *shape: pltpu.SemaphoreType.DMA(shape)
    return pl.pallas_call(
        layer_kernel,
        out_shape=(
            jax.ShapeDtypeStruct((ROWS, COLS), bf16),
            jax.ShapeDtypeStruct((128, COLS), bf16),
        ),
        in_specs=[hbm] * 5 + [smem] + [hbm] * 9,
        out_specs=(hbm, hbm),
        scratch_shapes=[
            V(ROWS, 256), V(ROWS, 256), V(ROWS, 256),
            F(ROWS, 128), F(ROWS, 128), F(1, 256), V(128, 2048), F(1, 2048),
            pltpu.VMEM((2, 128), jnp.int32), F(2, 128),
            V(256, ROWS), V(2, ROWS, ROWS), V(2, NZ, PAIR, COLS), V(2, 128, 2 * NZ * PAIR),
            F(2, 128, 128), V(ROWS, COLS), V(128, COLS),
            V(4 * NZ, ROWS, ROWS),
            pltpu.VMEM((2, ROWS, ROWS), f32),
            pltpu.VMEM((2, 1, ROWS), f32),
            pltpu.VMEM((2, 1, ROWS), f32),
            V(ROWS, 2048), V(2048, 256), V(2048, 256), V(256, 2048),
            V(NZ, PAIR, COLS), V(NZ, PAIR, COLS), V(NZ, PAIR, COLS),
            V(4, 4, HALF, PAIR, COLS), V(4, 4, HALF, PAIR, COLS),
            V(4, 4, n, COLS), V(4, 4, n, COLS), V(3, 4, n, COLS), V(3, 4, n, COLS),
            V(4, n, COLS), V(4, n, COLS), V(3, n, COLS), V(3, n, COLS),
            V(NZ, PAIR, COLS), V(2, NZ, PAIR, COLS),
            V(4, 4, h, COLS), V(4, 4, h, COLS), V(3, 4, h, COLS), V(3, 4, h, COLS),
            V(4, h, COLS), V(4, h, COLS), V(3, h, COLS), V(3, h, COLS),
            D(NZ, 2), D(NZ), D(3), D(2), D(2), D(1), D(1), D(1), D(1), D(6, 2), D(6, 2), D(16),
        ],
        compiler_params=pltpu.CompilerParams(
            collective_id=0, has_side_effects=True, vmem_limit_bytes=60 * 1024 * 1024
        ),
    )(*operands)


def on_device(
    query_maps, key_maps, value_rows, head_lambda, head_gain, out_weight,
    expert_rows, expert_gain, routes, route_weights, gate_weight, up_weight, down_weight,
):
    row_count = query_maps.shape[0]
    positions = lax.axis_index("ep") * row_count + jnp.arange(row_count, dtype=jnp.int32)
    half = jnp.arange(128, dtype=jnp.int32) % 64
    inverse = rope_base ** (-2.0 * half.astype(f32) / 128)
    angles = positions.astype(f32)[:, None] * inverse[None, :]
    sign = jnp.where(jnp.arange(128) < 64, -1.0, 1.0).astype(f32)
    return call_kernel(
        query_maps, key_maps, value_rows, jnp.cos(angles), jnp.sin(angles) * sign,
        head_lambda.reshape(1, 1), head_gain.reshape(1, -1), out_weight, expert_rows,
        expert_gain.reshape(1, -1), routes.T, route_weights.T,
        gate_weight[0], up_weight[0], down_weight[0],
    )


def solution(mesh):
    placed = (
        P("ep", "tp"),
        P("ep", "tp"),
        P("ep", "tp"),
        P("tp"),
        P(),
        P("tp", None),
        P("ep", None),
        P(),
        P("ep", None),
        P("ep", None),
        P("ep", None, "tp"),
        P("ep", None, "tp"),
        P("ep", "tp", None),
    )
    return jax.shard_map(
        on_device,
        mesh=mesh,
        in_specs=placed,
        out_specs=(P("ep", "tp"), P("ep", "tp")),
        check_vma=False,
    )
```

```python
import functools

import jax
import jax.numpy as jnp
import numpy as np
from jax import lax
from jax.experimental import pallas as pl
from jax.experimental.pallas import tpu as pltpu
from jax.sharding import PartitionSpec as P

norm_eps = 1e-06
rope_base = 10000.0
log2e = 1.4426950408889634

NZ = 16
NX = 4
NY = 4
SLOTS = 12
PAIR = 2 * SLOTS
HALF = NZ // 2
ROWS = 256
COLS = 128

MESH = pl.DeviceIdType.MESH
bf16 = jnp.bfloat16
f32 = jnp.float32


def layer_kernel(
    q_hbm, k_hbm, v_hbm, turns_hbm, lam, gain_hbm, wout_hbm, rows_hbm, rgain_hbm,
    routes_hbm, rweights_hbm, gate_hbm, up_hbm, down_hbm,
    mixed, expert_out,
    q_in, k_in, v_in, turns, cos_t, sin_t, gain, row_in, rgain, routes, rweights,
    q_t, kv_own, disp, pick, spread,
    kv, acc, run_max, run_sum, wout, gate_w, up_w, down_w,
    exch_in, z_send, z_in, ag, rs, rs_in, mid, fin,
    ret_send, ret, at_a, at_b, at_a_in, at_b_in, atm_a, atm_b, atf_a, atf_b,
    ring_recv, core_recv, kv_sent, pair_send, pair_recv,
    z_sent, z_came, ret_sent, ret_came, plane_send, plane_recv, tail_send, tail_recv, local_sem, known,
):
    ep = lax.axis_index("ep")
    tp = lax.axis_index("tp")
    z = ep // 2
    c = ep % 2
    y = tp // NX
    x = tp % NX
    partner = (z * 2 + 1 - c, tp)
    right = (((z + 1) % NZ) * 2 + c, tp)
    left = (((z + NZ - 1) % NZ) * 2 + c, tp)

    def z_peer(d):
        return (((z + d) % NZ) * 2 + c, tp)

    def x_peer(d):
        return (ep, y * NX + (x + d) % NX)

    def y_peer(d):
        return (ep, ((y + d) % NY) * NX + x)

    def remote(src, dst, send, recv, device):
        return pltpu.make_async_remote_copy(
            src_ref=src, dst_ref=dst, send_sem=send, recv_sem=recv,
            device_id=device, device_id_type=MESH,
        )

    loads = [
        pltpu.make_async_copy(src, dst, local_sem.at[i])
        for i, (src, dst) in enumerate(
            (
                (turns_hbm, turns), (k_hbm, k_in), (v_hbm, v_in),
                (rows_hbm, row_in), (routes_hbm, routes), (rgain_hbm, rgain), (q_hbm, q_in),
                (rweights_hbm, rweights), (gate_hbm, gate_w), (up_hbm, up_w),
                (down_hbm, down_w), (wout_hbm, wout), (gain_hbm, gain),
            )
        )
    ]

    barrier = pltpu.get_barrier_semaphore()
    for device in (z_peer(2), z_peer(NZ - 2), right, left, partner):
        pl.semaphore_signal(barrier, inc=1, device_id=device, device_id_type=MESH)
    for d in range(1, 4):
        pl.semaphore_signal(barrier, inc=1, device_id=x_peer(d), device_id_type=MESH)
        pl.semaphore_signal(barrier, inc=1, device_id=y_peer(d), device_id_type=MESH)
    for load in loads:
        load.start()

    def tell(i):
        for d in (2 ** (i + 1), NZ - 2 ** (i + 1)):
            pl.semaphore_signal(known.at[i], inc=1, device_id=z_peer(d), device_id_type=MESH)

    def learn(i):
        pl.semaphore_wait(known.at[i], 2)

    def turned(maps, m):
        wide = maps[:, m * 128:(m + 1) * 128].astype(f32)
        return wide * cos_t[...] + pltpu.roll(wide, 64, 1) * sin_t[...]

    loads[0].wait()
    lane = lax.broadcasted_iota(jnp.int32, (128, 128), 1)
    spot = lax.broadcasted_iota(jnp.int32, (128, 128), 0) + jnp.where(lane < 64, 0, 128)
    angles = (ep * ROWS + spot).astype(f32) * turns[...]
    for table, packed in ((cos_t, jnp.cos(angles)), (sin_t, jnp.sin(angles))):
        rolled = pltpu.roll(packed, 64, 1)
        low = -1.0 if table is sin_t else 1.0
        table[0:128] = jnp.where(lane < 64, packed * low, rolled)
        table[128:256] = jnp.where(lane < 64, rolled * low, packed)
    loads[1].wait()
    for m in range(2):
        kv_own[0, :, m * 128:(m + 1) * 128] = turned(k_in, m).astype(bf16)
    loads[2].wait()
    kv_own[1] = v_in[...].astype(f32).T.astype(bf16)
    pl.semaphore_wait(barrier, 5 + 6)
    tell(0)

    def ring_piece(chip, p):
        return kv.at[chip * 4 + c * 2 + p]

    def ring_wait(chip, p):
        here = ring_piece(chip, p)
        remote(here, here, kv_sent.at[0], ring_recv.at[chip, p], left).wait_recv()

    def core_wait(chip):
        here = kv.at[pl.ds(chip * 4 + 2 - c * 2, 2)]
        remote(here, here, kv_sent.at[2], core_recv.at[chip], partner).wait_recv()

    def ring_copy(src, chip, p, way, device):
        return remote(src, ring_piece(chip, p), kv_sent.at[way], ring_recv.at[chip, p], device)

    def core_copy(src, chip, p):
        return remote(src, ring_piece(chip, p), kv_sent.at[2], core_recv.at[chip], partner)

    def send_own(p):
        @pl.when(z < NZ - 1)
        def _():
            ring_copy(kv_own.at[p], z, p, 0, right).start()

        @pl.when(z <= 6 + p)
        def _():
            ring_copy(kv_own.at[p], z, p, 1, left).start()

        @pl.when(c == 0)
        def _():
            core_copy(kv_own.at[p], z, p).start()

    send_own(0)
    send_own(1)

    for i in range(3, 6):
        loads[i].wait()
    wide = row_in[...].astype(f32)
    level = lax.rsqrt(jnp.mean(wide * wide, axis=1, keepdims=True) + norm_eps)
    column = pl.ds(pl.multiple_of(tp * COLS, COLS), COLS)
    normed = (row_in[:, column].astype(f32) * level * rgain[:, column]).astype(bf16)
    chosen = [routes[k:k + 1, :] for k in range(2)]
    names = lax.broadcasted_iota(jnp.int32, (32, 128), 0)
    hot = [(names == r).astype(f32) for r in chosen]
    earlier = (
        lax.broadcasted_iota(jnp.int32, (128, 128), 0)
        < lax.broadcasted_iota(jnp.int32, (128, 128), 1)
    )
    counts = jnp.dot(
        (hot[0] + hot[1]).astype(bf16), earlier.astype(f32).astype(bf16),
        preferred_element_type=f32,
    )
    lines = lax.broadcasted_iota(jnp.int32, (2 * NZ * PAIR, 128), 0).astype(f32)
    base = [
        ((r // 2) * PAIR + c * SLOTS).astype(f32) + jnp.sum(counts * h, axis=0, keepdims=True)
        for r, h in zip(chosen, hot)
    ]
    block = float(NZ * PAIR)
    to_row = [b + (r % 2).astype(f32) * block for b, r in zip(base, chosen)]
    from_row = [
        b + jnp.where(r % 2 == c, 0.0, block) for b, r in zip(base, chosen)
    ]
    spot_of = jnp.where((lines == to_row[0]) | (lines == to_row[1]), 1.0, 0.0).astype(bf16)
    disp[...] = (
        jnp.dot(spot_of, normed, preferred_element_type=f32)
        .astype(bf16)
        .reshape(2, NZ, PAIR, COLS)
    )
    exch = remote(disp.at[1 - c], exch_in, pair_send.at[0], pair_recv.at[0], partner)
    exch.start()
    learn(0)
    tell(1)

    loads[6].wait()
    for m in range(2):
        q_t[m * 128:(m + 1) * 128, :] = turned(q_in, m).T.astype(bf16)
    exch.wait_recv()
    z_send[...] = (disp[c].astype(f32) + exch_in[...].astype(f32)).astype(bf16)
    z_in[z] = z_send[z]
    learn(1)
    for d in range(1, NZ):
        remote(
            z_send.at[(z + d) % NZ], z_in.at[z], z_sent.at[0], z_came.at[0], z_peer(d)
        ).start()
    loads[7].wait()
    for k in range(2):
        pick[k] = jnp.where(lines == from_row[k], 1.0, 0.0).T.astype(bf16)
        spread[k] = jnp.broadcast_to(rweights[k:k + 1, :], (128, 128)).T

    scale = (128 ** -0.5) * log2e

    def fold(k_of, v_of, count, masked, first):
        for m in range(2):
            q_m = q_t[m * 128:(m + 1) * 128, :]
            scores = []
            for i in range(count):
                s = jnp.dot(k_of(i)[:, m * 128:(m + 1) * 128], q_m, preferred_element_type=f32)
                if masked:
                    rows = lax.broadcasted_iota(jnp.int32, s.shape, 0)
                    cols = lax.broadcasted_iota(jnp.int32, s.shape, 1)
                    s = jnp.where(rows <= cols, s, -1e30)
                scores.append(s)
            top = jnp.max(scores[0], axis=0, keepdims=True)
            for s in scores[1:]:
                top = jnp.maximum(top, jnp.max(s, axis=0, keepdims=True))
            top = top * scale
            if first:
                new_max = top
            else:
                old = run_max[m]
                new_max = jnp.maximum(old, top)
                alpha = jnp.exp2(old - new_max)
            total = None
            out = None
            for i in range(count):
                e = jnp.exp2(scores[i] * scale - new_max)
                t = jnp.sum(e, axis=0, keepdims=True)
                total = t if total is None else total + t
                o = jnp.dot(v_of(i), e.astype(bf16), preferred_element_type=f32)
                out = o if out is None else out + o
            run_max[m] = new_max
            if first:
                run_sum[m] = total
                acc[m] = out
            else:
                run_sum[m] = run_sum[m] * alpha + total
                acc[m] = acc[m] * alpha + out

    fold(lambda i: kv_own[0], lambda i: kv_own[1], 1, True, True)

    @pl.when(c == 1)
    def _():
        core_wait(z)
        fold(lambda i: kv[z * 4], lambda i: kv[z * 4 + 1], 1, False, False)

    def fold_chip(chip):
        core_wait(chip)
        fold(
            lambda i: kv[chip * 4 + i * 2], lambda i: kv[chip * 4 + i * 2 + 1], 2, False, False
        )

    place = [(y, x), (x, y)]
    first_peer = (x_peer, y_peer)
    second_peer = (y_peer, x_peer)

    def group_send(phase, g, src_of, dst_of, peer):
        for d in range(1, 4):
            remote(
                src_of(d), dst_of(d), plane_send.at[phase, g], plane_recv.at[phase, g], peer(d)
            ).start()

    def group_three(phase, g, ref):
        return remote(ref, ref, plane_send.at[phase, g], plane_recv.at[phase, g], partner)

    def tail_send_all(phase, half, src_of, dst_of, peer):
        for d in range(1, 4):
            remote(
                src_of(d), dst_of(d), tail_send.at[phase, half], tail_recv.at[phase, half], peer(d)
            ).start()

    def tail_three(phase, half, ref):
        return remote(ref, ref, tail_send.at[phase, half], tail_recv.at[phase, half], partner)

    few = pl.ds(0, 3)

    def gather_one():
        most = pl.ds(0, NZ - 1)
        remote(
            z_send.at[most], z_in.at[most], z_sent.at[0], z_came.at[0], partner
        ).wait_recv()
        for g in range(4):
            u, v = place[g % 2]
            block = pl.ds(4 * g, 4)
            ag[g, u, v] = z_in[block]
            group_send(
                0, g, lambda d: z_in.at[block], lambda d: ag.at[g, u, v], first_peer[g % 2]
            )

    def gather_two():
        for g in range(4):
            u, v = place[g % 2]
            group_three(0, g, ag.at[g, 0, few]).wait_recv()
            group_send(
                1, g, lambda d: ag.at[g, u], lambda d: ag.at[g, u], second_peer[g % 2]
            )

    n = 4 * PAIR

    def expert(r):
        if r == 0:
            for load in loads[8:11]:
                load.wait()
        for g in (2 * r, 2 * r + 1):
            group_three(1, g, ag.at[g, few]).wait_recv()
        pieces = [
            jnp.concatenate(
                [ag[2 * r, i, j].reshape(n, COLS), ag[2 * r + 1, j, i].reshape(n, COLS)], axis=0
            )
            for i in range(NY)
            for j in range(NX)
        ]
        rows = jnp.concatenate(pieces, axis=1)
        gates = jnp.dot(rows, gate_w[...], preferred_element_type=f32)
        ups = jnp.dot(rows, up_w[...], preferred_element_type=f32)
        hidden = (gates / (1.0 + jnp.exp(-gates)) * ups).astype(bf16)
        for i in range(NY):
            for j in range(NX):
                at = (i * NX + j) * COLS
                part = jnp.dot(
                    hidden, down_w[:, at:at + COLS], preferred_element_type=f32
                ).astype(bf16)
                rs[2 * r, i, j] = part[:n]
                rs[2 * r + 1, j, i] = part[n:]
        for g in (2 * r, 2 * r + 1):
            u, v = place[g % 2]
            group_send(
                2, g, lambda d: rs.at[g, (u + d) % 4], lambda d: rs_in.at[g, d - 1],
                second_peer[g % 2],
            )

    def sum_one(r):
        for g in (2 * r, 2 * r + 1):
            u, v = place[g % 2]
            group_three(2, g, rs_in.at[g]).wait_recv()
            for j in range(4):
                t = rs[g, u, j].astype(f32)
                for d in range(3):
                    t = t + rs_in[g, d, j].astype(f32)
                mid[g, j] = t.astype(bf16)
            group_send(
                3, g, lambda d: mid.at[g, (v + d) % 4], lambda d: fin.at[g, d - 1],
                first_peer[g % 2],
            )

    def sum_two(r):
        for g in (2 * r, 2 * r + 1):
            u, v = place[g % 2]
            group_three(3, g, fin.at[g]).wait_recv()
            t = mid[g, v].astype(f32)
            for d in range(3):
                t = t + fin[g, d].astype(f32)
            ret_send[4 * g:4 * g + 4] = t.astype(bf16).reshape(4, PAIR, COLS)
        for to in range(HALF * r, HALF * (r + 1)):
            @pl.when(z == to)
            def _():
                ret[0, to] = ret_send[to]

            @pl.when(z != to)
            def _():
                remote(
                    ret_send.at[to], ret.at[0, z], ret_sent.at[0], ret_came.at[0],
                    (to * 2 + c, tp),
                ).start()

    def tick(s, carry):
        zl = jnp.maximum(z - s, 0)
        zr = (z + s) % NZ
        wrapped = z + s >= NZ

        def plus(p, last):
            @pl.when((s <= last) & (s <= z))
            def _():
                ring_wait(zl, p)

                @pl.when((z < NZ - 1) & (s < last))
                def _():
                    ring_copy(ring_piece(zl, p), zl, p, 0, right).start()

                core_copy(ring_piece(zl, p), zl, p).start()

        def minus(p, last):
            @pl.when((s <= last) & (zr <= 6 + p))
            def _():
                ring_wait(zr, p)

                @pl.when(s < last)
                def _():
                    ring_copy(ring_piece(zr, p), zr, p, 1, left).start()

                @pl.when(wrapped)
                def _():
                    core_copy(ring_piece(zr, p), zr, p).start()

        def fold_minus():
            @pl.when((s >= 2) & (s - 1 <= 7) & (z + s - 1 >= NZ))
            def _():
                fold_chip(jnp.maximum(z + s - 1 - NZ, 0))

        plus(0, 8)
        minus(0, 7)

        @pl.when(s == 5)
        def _():
            expert(0)

        @pl.when(s == 7)
        def _():
            sum_one(0)

        @pl.when(s == 8)
        def _():
            sum_two(0)

        @pl.when(s == 9)
        def _():
            sum_two(1)

        @pl.when((s >= 2) & (s - 1 <= z))
        def _():
            fold_chip(jnp.maximum(z - s + 1, 0))

        @pl.when(s == 8)
        def _():
            fold_minus()

        plus(1, 7)
        minus(1, 8)

        @pl.when(s == 2)
        def _():
            gather_one()

        @pl.when(s == 3)
        def _():
            gather_two()

        @pl.when(s == 5)
        def _():
            expert(1)

        @pl.when(s == 7)
        def _():
            sum_one(1)

        @pl.when(s < 8)
        def _():
            fold_minus()

        return carry

    lax.fori_loop(1, 10, tick, 0)

    first = acc[0] / run_sum[0]
    second = acc[1] / run_sum[1]
    diff = first - lam[0, 0] * second
    mean = jnp.mean(diff * diff, axis=0, keepdims=True)
    head_t = diff * lax.rsqrt(mean + norm_eps)
    for load in loads[11:13]:
        load.wait()
    head = (head_t.T * gain[...]).astype(bf16)
    for i in range(NY):
        for j in range(NX):
            at = (i * NX + j) * COLS
            part = jnp.dot(head, wout[:, at:at + COLS], preferred_element_type=f32).astype(bf16)
            at_a[i, j] = part[:ROWS // 2]
            at_b[j, i] = part[ROWS // 2:]
    tail_send_all(
        0, 0, lambda d: at_a.at[(y + d) % NY], lambda d: at_a_in.at[d - 1], y_peer
    )
    tail_send_all(
        0, 1, lambda d: at_b.at[(x + d) % NX], lambda d: at_b_in.at[d - 1], x_peer
    )

    tail_three(0, 0, at_a_in).wait_recv()
    for j in range(4):
        t = at_a[y, j].astype(f32)
        for d in range(3):
            t = t + at_a_in[d, j].astype(f32)
        atm_a[j] = t.astype(bf16)
    tail_send_all(
        1, 0, lambda d: atm_a.at[(x + d) % NX], lambda d: atf_a.at[d - 1], x_peer
    )
    tail_three(0, 1, at_b_in).wait_recv()
    for j in range(4):
        t = at_b[x, j].astype(f32)
        for d in range(3):
            t = t + at_b_in[d, j].astype(f32)
        atm_b[j] = t.astype(bf16)
    tail_send_all(
        1, 1, lambda d: atm_b.at[(y + d) % NY], lambda d: atf_b.at[d - 1], y_peer
    )

    most = pl.ds(0, NZ - 1)
    remote(
        ret_send.at[most], ret.at[0, most], ret_sent.at[0], ret_came.at[0], partner
    ).wait_recv()
    back = remote(ret.at[0], ret.at[1], pair_send.at[1], pair_recv.at[1], partner)
    back.start()

    back.wait_recv()
    rows = ret[...].reshape(2 * NZ * PAIR, COLS)
    mixture = jnp.dot(pick[0], rows, preferred_element_type=f32) * spread[0]
    mixture = mixture + jnp.dot(pick[1], rows, preferred_element_type=f32) * spread[1]
    expert_out[...] = mixture.astype(bf16)

    tail_three(1, 0, atf_a).wait_recv()
    t = atm_a[x].astype(f32)
    for d in range(3):
        t = t + atf_a[d].astype(f32)
    mixed[0:ROWS // 2] = t.astype(bf16)
    tail_three(1, 1, atf_b).wait_recv()
    t = atm_b[y].astype(f32)
    for d in range(3):
        t = t + atf_b[d].astype(f32)
    mixed[ROWS // 2:ROWS] = t.astype(bf16)

    exch.wait_send()
    back.wait_send()
    remote(z_send.at[most], z_in.at[most], z_sent.at[0], z_came.at[0], partner).wait_send()
    remote(
        ret_send.at[most], ret.at[0, most], ret_sent.at[0], ret_came.at[0], partner
    ).wait_send()
    for g in range(4):
        group_three(0, g, ag.at[g, 0, few]).wait_send()
        group_three(1, g, ag.at[g, few]).wait_send()
        group_three(2, g, rs_in.at[g]).wait_send()
        group_three(3, g, fin.at[g]).wait_send()
    for half in range(2):
        tail_three(0, half, at_a_in).wait_send()
        tail_three(1, half, atf_a).wait_send()

    def sent(way, count):
        if count:
            here = kv.at[pl.ds(0, count)]
            remote(here, here, kv_sent.at[way], core_recv.at[0], partner).wait_send()

    for at in range(NZ):
        @pl.when(z == at)
        def _():
            came_plus = [min(at, 8 - p) for p in range(2)]
            on_plus = [0 if at == NZ - 1 else 1 + min(at, 7 - p) for p in range(2)]
            on_minus = [
                sum((at + s) % NZ <= 6 + p for s in range(7 + p)) for p in range(2)
            ]
            wrapped = [
                sum((at + s) % NZ <= 6 + p and at + s >= NZ for s in range(1, 8 + p))
                for p in range(2)
            ]
            sent(0, sum(on_plus))
            sent(1, sum(on_minus))
            passed = sum(came_plus) + sum(wrapped)

            @pl.when(c == 0)
            def _():
                sent(2, passed + 2)

            @pl.when(c == 1)
            def _():
                sent(2, passed)


def call_kernel(*operands):
    vmem = pl.BlockSpec(memory_space=pltpu.VMEM)
    hbm = pl.BlockSpec(memory_space=pl.ANY)
    smem = pl.BlockSpec(memory_space=pltpu.SMEM)
    n = 4 * PAIR
    h = ROWS // 2
    V = lambda *shape: pltpu.VMEM(shape, bf16)
    F = lambda *shape: pltpu.VMEM(shape, f32)
    D = lambda *shape: pltpu.SemaphoreType.DMA(shape)
    return pl.pallas_call(
        layer_kernel,
        out_shape=(
            pltpu.VMEM((ROWS, COLS), bf16),
            pltpu.VMEM((128, COLS), bf16),
        ),
        in_specs=[hbm] * 4 + [smem] + [hbm] * 9,
        out_specs=(vmem, vmem),
        scratch_shapes=[
            V(ROWS, 256), V(ROWS, 256), V(ROWS, 256),
            F(1, 128), F(ROWS, 128), F(ROWS, 128), F(1, 256), V(128, 2048), F(1, 2048),
            pltpu.VMEM((2, 128), jnp.int32), F(2, 128),
            V(256, ROWS), V(2, ROWS, ROWS), V(2, NZ, PAIR, COLS), V(2, 128, 2 * NZ * PAIR),
            F(2, 128, 128),
            V(4 * NZ, ROWS, ROWS),
            pltpu.VMEM((2, ROWS, ROWS), f32),
            pltpu.VMEM((2, 1, ROWS), f32),
            pltpu.VMEM((2, 1, ROWS), f32),
            V(ROWS, 2048), V(2048, 256), V(2048, 256), V(256, 2048),
            V(NZ, PAIR, COLS), V(NZ, PAIR, COLS), V(NZ, PAIR, COLS),
            V(4, 4, 4, 4, PAIR, COLS), V(4, 4, 4, n, COLS), V(4, 3, 4, n, COLS),
            V(4, 4, n, COLS), V(4, 3, n, COLS),
            V(NZ, PAIR, COLS), V(2, NZ, PAIR, COLS),
            V(4, 4, h, COLS), V(4, 4, h, COLS), V(3, 4, h, COLS), V(3, 4, h, COLS),
            V(4, h, COLS), V(4, h, COLS), V(3, h, COLS), V(3, h, COLS),
            D(NZ, 2), D(NZ), D(3), D(2), D(2), D(1), D(1), D(1), D(1), D(4, 4), D(4, 4), D(2, 2), D(2, 2), D(13),
            pltpu.SemaphoreType.REGULAR((2,)),
        ],
        compiler_params=pltpu.CompilerParams(
            collective_id=0, has_side_effects=True, vmem_limit_bytes=60 * 1024 * 1024
        ),
    )(*operands)


def on_device(
    query_maps, key_maps, value_rows, head_lambda, head_gain, out_weight,
    expert_rows, expert_gain, routes, route_weights, gate_weight, up_weight, down_weight,
):
    turns = rope_base ** (-2.0 * (np.arange(128) % 64) / 128)
    return call_kernel(
        query_maps, key_maps, value_rows, jnp.asarray(turns[None], f32),
        head_lambda.reshape(1, 1), head_gain.reshape(1, -1), out_weight, expert_rows,
        expert_gain.reshape(1, -1), routes.T, route_weights.T,
        gate_weight[0], up_weight[0], down_weight[0],
    )


def solution(mesh):
    placed = (
        P("ep", "tp"),
        P("ep", "tp"),
        P("ep", "tp"),
        P("tp"),
        P(),
        P("tp", None),
        P("ep", None),
        P(),
        P("ep", None),
        P("ep", None),
        P("ep", None, "tp"),
        P("ep", None, "tp"),
        P("ep", "tp", None),
    )
    return jax.shard_map(
        on_device,
        mesh=mesh,
        in_specs=placed,
        out_specs=(P("ep", "tp"), P("ep", "tp")),
        check_vma=False,
    )
```

```python
import functools

import jax
import jax.numpy as jnp
import numpy as np
from jax import lax
from jax.experimental import pallas as pl
from jax.experimental.pallas import tpu as pltpu
from jax.sharding import PartitionSpec as P

norm_eps = 1e-06
rope_base = 10000.0
log2e = 1.4426950408889634

NZ = 16
NX = 4
NY = 4
SLOTS = 12
PAIR = 2 * SLOTS
HALF = NZ // 2
ROWS = 256
COLS = 128

MESH = pl.DeviceIdType.MESH
bf16 = jnp.bfloat16
f32 = jnp.float32


def layer_kernel(
    q_hbm, k_hbm, v_hbm, turns_hbm, lam_hbm, gain_hbm, wout_hbm, rows_hbm, rgain_hbm,
    routes_hbm, rweights_hbm, gate_hbm, up_hbm, down_hbm,
    mixed, expert_out,
    q_in, k_in, v_in, turns, cos_t, sin_t, lam, gain, row_in, rgain, routes, rweights,
    q_t, kv_own, disp, pick, spread, weights,
    kv, acc, run_max, run_sum, wout, gate_w, up_w, down_w,
    exch_in, z_send, z_in, ag, rs, rs_in, mid, fin,
    ret_send, ret, tail, tail_in, tail_mid, tail_fin,
    ring_recv, core_recv, kv_sent, pair_send, pair_recv,
    z_sent, z_came, ret_sent, ret_came, plane_send, plane_recv, tail_send, tail_recv, local_sem, known,
):
    ep = lax.axis_index("ep")
    tp = lax.axis_index("tp")
    z = ep // 2
    c = ep % 2
    y = tp // NX
    x = tp % NX
    partner = (z * 2 + 1 - c, tp)
    right = (((z + 1) % NZ) * 2 + c, tp)
    left = (((z + NZ - 1) % NZ) * 2 + c, tp)

    def z_peer(d):
        return (((z + d) % NZ) * 2 + c, tp)

    def x_peer(d):
        return (ep, y * NX + (x + d) % NX)

    def y_peer(d):
        return (ep, ((y + d) % NY) * NX + x)

    def remote(src, dst, send, recv, device):
        return pltpu.make_async_remote_copy(
            src_ref=src, dst_ref=dst, send_sem=send, recv_sem=recv,
            device_id=device, device_id_type=MESH,
        )

    loads = [
        pltpu.make_async_copy(src, dst, local_sem.at[i])
        for i, (src, dst) in enumerate(
            (
                (turns_hbm, turns), (k_hbm, k_in), (v_hbm, v_in),
                (rows_hbm, row_in), (routes_hbm, routes), (rgain_hbm, rgain), (q_hbm, q_in),
                (rweights_hbm, rweights), (gate_hbm, gate_w), (up_hbm, up_w),
                (down_hbm, down_w), (wout_hbm, wout), (gain_hbm, gain), (lam_hbm, lam),
            )
        )
    ]

    barrier = pltpu.get_barrier_semaphore()
    for device in (z_peer(2), z_peer(NZ - 2), right, left, partner):
        pl.semaphore_signal(barrier, inc=1, device_id=device, device_id_type=MESH)
    for d in range(1, 4):
        pl.semaphore_signal(barrier, inc=1, device_id=x_peer(d), device_id_type=MESH)
        pl.semaphore_signal(barrier, inc=1, device_id=y_peer(d), device_id_type=MESH)
    for load in loads:
        load.start()

    def tell(i):
        for d in (2 ** (i + 1), NZ - 2 ** (i + 1)):
            pl.semaphore_signal(known.at[i], inc=1, device_id=z_peer(d), device_id_type=MESH)

    def learn(i):
        pl.semaphore_wait(known.at[i], 2)

    def turned(maps, m):
        wide = maps[:, m * 128:(m + 1) * 128].astype(f32)
        return wide * cos_t[...] + pltpu.roll(wide, 64, 1) * sin_t[...]

    loads[0].wait()
    pl.semaphore_wait(barrier, 5 + 6)
    tell(0)
    lane = lax.broadcasted_iota(jnp.int32, (128, 128), 1)
    spot = lax.broadcasted_iota(jnp.int32, (128, 128), 0) + jnp.where(lane < 64, 0, 128)
    angles = (ep * ROWS + spot).astype(f32) * turns[...]
    for table, packed in ((cos_t, jnp.cos(angles)), (sin_t, jnp.sin(angles))):
        rolled = pltpu.roll(packed, 64, 1)
        low = -1.0 if table is sin_t else 1.0
        table[0:128] = jnp.where(lane < 64, packed * low, rolled)
        table[128:256] = jnp.where(lane < 64, rolled * low, packed)
    loads[1].wait()
    for m in range(2):
        kv_own[0, :, m * 128:(m + 1) * 128] = turned(k_in, m).astype(bf16)
    loads[2].wait()
    kv_own[1] = v_in[...].astype(f32).T.astype(bf16)

    def ring_piece(chip, p):
        return kv.at[chip * 4 + c * 2 + p]

    def ring_wait(chip, p):
        here = ring_piece(chip, p)
        remote(here, here, kv_sent.at[0], ring_recv.at[chip, p], left).wait_recv()

    def core_wait(chip):
        here = kv.at[pl.ds(chip * 4 + 2 - c * 2, 2)]
        remote(here, here, kv_sent.at[2], core_recv.at[chip], partner).wait_recv()

    def core_wait_one(chip, p, mark):
        here = kv.at[chip * 4 + 2 - c * 2 + p]
        remote(here, here, kv_sent.at[2], core_recv.at[mark], partner).wait_recv()

    def ring_copy(src, chip, p, way, device):
        return remote(src, ring_piece(chip, p), kv_sent.at[way], ring_recv.at[chip, p], device)

    def core_copy(src, chip, p, mark):
        return remote(src, ring_piece(chip, p), kv_sent.at[2], core_recv.at[mark], partner)

    def send_own(p):
        @pl.when(z < NZ - 1)
        def _():
            ring_copy(kv_own.at[p], z, p, 0, right).start()

        @pl.when(z <= 6 + p)
        def _():
            ring_copy(kv_own.at[p], z, p, 1, left).start()

        @pl.when(c == 0)
        def _():
            core_copy(kv_own.at[p], z, p, z).start()

    send_own(0)
    send_own(1)

    for i in range(3, 6):
        loads[i].wait()
    wide = row_in[...].astype(f32)
    level = lax.rsqrt(jnp.mean(wide * wide, axis=1, keepdims=True) + norm_eps)
    column = pl.ds(pl.multiple_of(tp * COLS, COLS), COLS)
    normed = (row_in[:, column].astype(f32) * level * rgain[:, column]).astype(bf16)
    chosen = [routes[k:k + 1, :] for k in range(2)]
    names = lax.broadcasted_iota(jnp.int32, (32, 128), 0)
    hot = [(names == r).astype(f32) for r in chosen]
    earlier = (
        lax.broadcasted_iota(jnp.int32, (128, 128), 0)
        < lax.broadcasted_iota(jnp.int32, (128, 128), 1)
    )
    counts = jnp.dot(
        (hot[0] + hot[1]).astype(bf16), earlier.astype(f32).astype(bf16),
        preferred_element_type=f32,
    )
    lines = lax.broadcasted_iota(jnp.int32, (2 * NZ * PAIR, 128), 0).astype(f32)
    base = [
        ((r // 2) * PAIR + c * SLOTS).astype(f32) + jnp.sum(counts * h, axis=0, keepdims=True)
        for r, h in zip(chosen, hot)
    ]
    block = float(NZ * PAIR)
    to_row = [b + (r % 2).astype(f32) * block for b, r in zip(base, chosen)]
    from_row = [
        b + jnp.where(r % 2 == c, 0.0, block) for b, r in zip(base, chosen)
    ]
    spot_of = jnp.where((lines == to_row[0]) | (lines == to_row[1]), 1.0, 0.0).astype(bf16)
    disp[...] = (
        jnp.dot(spot_of, normed, preferred_element_type=f32)
        .astype(bf16)
        .reshape(2, NZ, PAIR, COLS)
    )
    exch = remote(disp.at[1 - c], exch_in, pair_send.at[0], pair_recv.at[0], partner)
    exch.start()
    learn(0)
    tell(1)

    loads[6].wait()
    for m in range(2):
        q_t[m * 128:(m + 1) * 128, :] = turned(q_in, m).T.astype(bf16)
    exch.wait_recv()
    z_send[...] = (disp[c].astype(f32) + exch_in[...].astype(f32)).astype(bf16)
    z_in[z] = z_send[z]

    def dispatch():
        learn(1)
        for d in range(1, NZ):
            remote(
                z_send.at[(z + d) % NZ], z_in.at[z], z_sent.at[0], z_came.at[0], z_peer(d)
            ).start()

    loads[7].wait()
    for k in range(2):
        pick[k] = jnp.where(lines == from_row[k], 1.0, 0.0).T.astype(bf16)
        spread[k] = jnp.broadcast_to(rweights[k:k + 1, :], (128, 128)).T

    scale = (128 ** -0.5) * log2e

    def fold(k_of, v_of, count, masked, first, later=False):
        for m in range(2):
            q_m = q_t[m * 128:(m + 1) * 128, :]
            scores = []
            for i in range(count):
                s = jnp.dot(k_of(i)[:, m * 128:(m + 1) * 128], q_m, preferred_element_type=f32)
                if masked:
                    rows = lax.broadcasted_iota(jnp.int32, s.shape, 0)
                    cols = lax.broadcasted_iota(jnp.int32, s.shape, 1)
                    s = jnp.where(rows <= cols, s, -1e30)
                scores.append(s)
            top = jnp.max(scores[0], axis=0, keepdims=True)
            for s in scores[1:]:
                top = jnp.maximum(top, jnp.max(s, axis=0, keepdims=True))
            top = top * scale
            if first:
                new_max = top
            else:
                old = run_max[m]
                new_max = jnp.maximum(old, top)
                alpha = jnp.exp2(old - new_max)
            total = None
            out = None
            for i in range(count):
                e = jnp.exp2(scores[i] * scale - new_max)
                t = jnp.sum(e, axis=0, keepdims=True)
                total = t if total is None else total + t
                if later:
                    weights[m, i] = e.astype(bf16)
                else:
                    o = jnp.dot(v_of(i), e.astype(bf16), preferred_element_type=f32)
                    out = o if out is None else out + o
            run_max[m] = new_max
            if first:
                run_sum[m] = total
                acc[m] = out
            else:
                run_sum[m] = run_sum[m] * alpha + total
                acc[m] = acc[m] * alpha if later else acc[m] * alpha + out

    fold(lambda i: kv_own[0], lambda i: kv_own[1], 1, True, True)

    @pl.when(c == 1)
    def _():
        core_wait(z)
        fold(lambda i: kv[z * 4], lambda i: kv[z * 4 + 1], 1, False, False)

    def fold_chip(chip):
        core_wait(chip)
        fold(
            lambda i: kv[chip * 4 + i * 2], lambda i: kv[chip * 4 + i * 2 + 1], 2, False, False
        )

    place = [(y, x), (x, y)]
    first_peer = (x_peer, y_peer)
    second_peer = (y_peer, x_peer)

    def group_send(phase, g, src_of, dst_of, peer):
        for d in range(1, 4):
            remote(
                src_of(d), dst_of(d), plane_send.at[phase], plane_recv.at[phase, g], peer(d)
            ).start()

    def group_three(phase, g, ref):
        return remote(ref, ref, plane_send.at[phase], plane_recv.at[phase, g], partner)

    def tail_group(phase, g, src_of, dst_of, peer):
        for d in range(1, 4):
            remote(
                src_of(d), dst_of(d), tail_send.at[phase], tail_recv.at[phase, g], peer(d)
            ).start()

    def tail_three(phase, g, ref):
        return remote(ref, ref, tail_send.at[phase], tail_recv.at[phase, g], partner)

    few = pl.ds(0, 3)

    def gather_one():
        most = pl.ds(0, NZ - 1)
        remote(
            z_send.at[most], z_in.at[most], z_sent.at[0], z_came.at[0], partner
        ).wait_recv()
        for g in range(4):
            u, v = place[g % 2]
            block = pl.ds(4 * g, 4)
            ag[g, u, v] = z_in[block]
            group_send(
                0, g, lambda d: z_in.at[block], lambda d: ag.at[g, u, v], first_peer[g % 2]
            )

    def gather_two():
        for g in range(4):
            u, v = place[g % 2]
            group_three(0, g, ag.at[g, 0, few]).wait_recv()
            group_send(
                1, g, lambda d: ag.at[g, u], lambda d: ag.at[g, u], second_peer[g % 2]
            )

    n = 4 * PAIR

    def expert(r):
        if r == 0:
            for load in loads[8:11]:
                load.wait()
        for g in (2 * r, 2 * r + 1):
            group_three(1, g, ag.at[g, few]).wait_recv()
        pieces = [
            jnp.concatenate(
                [ag[2 * r, i, j].reshape(n, COLS), ag[2 * r + 1, j, i].reshape(n, COLS)], axis=0
            )
            for i in range(NY)
            for j in range(NX)
        ]
        rows = jnp.concatenate(pieces, axis=1)
        gates = jnp.dot(rows, gate_w[...], preferred_element_type=f32)
        ups = jnp.dot(rows, up_w[...], preferred_element_type=f32)
        hidden = (gates / (1.0 + jnp.exp(-gates)) * ups).astype(bf16)
        for i in range(NY):
            for j in range(NX):
                at = (i * NX + j) * COLS
                part = jnp.dot(
                    hidden, down_w[:, at:at + COLS], preferred_element_type=f32
                ).astype(bf16)
                rs[2 * r, i, j] = part[:n]
                rs[2 * r + 1, j, i] = part[n:]
        for g in (2 * r, 2 * r + 1):
            u, v = place[g % 2]
            group_send(
                2, g, lambda d: rs.at[g, (u + d) % 4], lambda d: rs_in.at[g, d - 1],
                second_peer[g % 2],
            )

    def sum_one(r):
        for g in (2 * r, 2 * r + 1):
            u, v = place[g % 2]
            group_three(2, g, rs_in.at[g]).wait_recv()
            for j in range(4):
                t = rs[g, u, j].astype(f32)
                for d in range(3):
                    t = t + rs_in[g, d, j].astype(f32)
                mid[g, j] = t.astype(bf16)
            group_send(
                3, g, lambda d: mid.at[g, (v + d) % 4], lambda d: fin.at[g, d - 1],
                first_peer[g % 2],
            )

    def sum_two(g):
        u, v = place[g % 2]
        group_three(3, g, fin.at[g]).wait_recv()
        t = mid[g, v].astype(f32)
        for d in range(3):
            t = t + fin[g, d].astype(f32)
        ret_send[4 * g:4 * g + 4] = t.astype(bf16).reshape(4, PAIR, COLS)
        for to in range(4 * g, 4 * g + 4):
            @pl.when(z == to)
            def _():
                ret[0, to] = ret_send[to]

            @pl.when(z != to)
            def _():
                remote(
                    ret_send.at[to], ret.at[0, z], ret_sent.at[0], ret_came.at[0],
                    (to * 2 + c, tp),
                ).start()

    def tick(s, carry):
        zl = jnp.maximum(z - s, 0)
        zr = (z + s) % NZ
        wrapped = z + s >= NZ

        def plus(p, last):
            @pl.when((s <= last) & (s <= z))
            def _():
                ring_wait(zl, p)

                @pl.when((z < NZ - 1) & (s < last))
                def _():
                    ring_copy(ring_piece(zl, p), zl, p, 0, right).start()

                core_copy(ring_piece(zl, p), zl, p, zl).start()

        def minus(p, last):
            @pl.when((s <= last) & (zr <= 6 + p))
            def _():
                ring_wait(zr, p)

                @pl.when(s < last)
                def _():
                    ring_copy(ring_piece(zr, p), zr, p, 1, left).start()

                @pl.when(wrapped)
                def _():
                    mark = jnp.where(s == 8, NZ, zr)
                    core_copy(ring_piece(zr, p), zr, p, mark).start()

        def fold_minus():
            @pl.when((s >= 2) & (s - 1 <= 7) & (z + s - 1 >= NZ))
            def _():
                fold_chip(jnp.maximum(z + s - 1 - NZ, 0))

        @pl.when(s == 5)
        def _():
            expert(0)

        plus(0, 8)
        minus(0, 7)

        @pl.when(s == 1)
        def _():
            dispatch()

        @pl.when(s == 7)
        def _():
            sum_one(1)

        @pl.when((s == 7) & (z >= 8))
        def _():
            sum_two(0)

        @pl.when((s >= 2) & (s - 1 <= z))
        def _():
            fold_chip(jnp.maximum(z - s + 1, 0))

        @pl.when(s == 8)
        def _():
            fold_minus()

        @pl.when(s == 6)
        def _():
            sum_one(0)

        @pl.when((s == 8) & (z >= 8))
        def _():
            far = jnp.maximum(z - 8, 0)
            core_wait_one(far, 0, far)
            fold(lambda i: kv[far * 4 + i * 2], None, 2, False, False, later=True)

        plus(1, 7)
        minus(1, 8)

        @pl.when(s == 2)
        def _():
            gather_one()

        @pl.when(s == 3)
        def _():
            gather_two()

        @pl.when(s == 5)
        def _():
            expert(1)

        @pl.when(s < 8)
        def _():
            fold_minus()

        return carry

    lax.fori_loop(1, 9, tick, 0)

    @pl.when(z >= 8)
    def _():
        sum_two(1)
        sum_two(2)
        sum_two(3)
        far = jnp.maximum(z - 8, 0)
        core_wait_one(far, 1, NZ)
        for m in range(2):
            out = jnp.dot(kv[far * 4 + 1], weights[m, 0], preferred_element_type=f32)
            acc[m] = acc[m] + (
                out + jnp.dot(kv[far * 4 + 3], weights[m, 1], preferred_element_type=f32)
            )


    @pl.when(z < 8)
    def _():
        sum_two(0)
        sum_two(1)

    for load in loads[11:14]:
        load.wait()
    first = acc[0] / run_sum[0]
    second = acc[1] / run_sum[1]
    diff = first - lam[...] * second
    mean = jnp.mean(diff * diff, axis=0, keepdims=True)
    head_t = diff * lax.rsqrt(mean + norm_eps)
    for half in range(2):
        head = (head_t[:, half * 128:(half + 1) * 128].T * gain[...]).astype(bf16)
        for i in range(NY):
            for j in range(NX):
                at = (i * NX + j) * COLS
                part = jnp.dot(
                    head, wout[:, at:at + COLS], preferred_element_type=f32
                ).astype(bf16)
                tail[2 * half, i, j] = part[:64]
                tail[2 * half + 1, j, i] = part[64:]
        for g in (2 * half, 2 * half + 1):
            u, v = place[g % 2]
            tail_group(
                0, g, lambda d: tail.at[g, (u + d) % 4], lambda d: tail_in.at[g, d - 1],
                second_peer[g % 2],
            )

    for g in range(4):
        u, v = place[g % 2]
        tail_three(0, g, tail_in.at[g]).wait_recv()
        for j in range(4):
            t = tail[g, u, j].astype(f32)
            for d in range(3):
                t = t + tail_in[g, d, j].astype(f32)
            tail_mid[g, j] = t.astype(bf16)
        tail_group(
            1, g, lambda d: tail_mid.at[g, (v + d) % 4], lambda d: tail_fin.at[g, d - 1],
            first_peer[g % 2],
        )
        if g == 1:
            @pl.when(z < 8)
            def _():
                sum_two(2)
                sum_two(3)

    most = pl.ds(0, NZ - 1)
    remote(
        ret_send.at[most], ret.at[0, most], ret_sent.at[0], ret_came.at[0], partner
    ).wait_recv()
    back = remote(ret.at[0], ret.at[1], pair_send.at[1], pair_recv.at[1], partner)
    back.start()

    back.wait_recv()
    rows = ret[...].reshape(2 * NZ * PAIR, COLS)
    mixture = jnp.dot(pick[0], rows, preferred_element_type=f32) * spread[0]
    mixture = mixture + jnp.dot(pick[1], rows, preferred_element_type=f32) * spread[1]
    expert_out[...] = mixture.astype(bf16)

    for g in range(4):
        tail_three(1, g, tail_fin.at[g]).wait_recv()
        t = tail_mid[g, place[g % 2][1]].astype(f32)
        for d in range(3):
            t = t + tail_fin[g, d].astype(f32)
        mixed[64 * g:64 * (g + 1)] = t.astype(bf16)

    exch.wait_send()
    back.wait_send()
    remote(z_send.at[most], z_in.at[most], z_sent.at[0], z_came.at[0], partner).wait_send()
    remote(
        ret_send.at[most], ret.at[0, most], ret_sent.at[0], ret_came.at[0], partner
    ).wait_send()
    group_three(0, 0, ag.at[0, few]).wait_send()
    group_three(1, 0, ag.at[few]).wait_send()
    group_three(2, 0, rs_in).wait_send()
    group_three(3, 0, fin).wait_send()
    tail_three(0, 0, tail_in).wait_send()
    tail_three(1, 0, tail_fin).wait_send()

    def sent(way, count):
        if count:
            here = kv.at[pl.ds(0, count)]
            remote(here, here, kv_sent.at[way], core_recv.at[0], partner).wait_send()

    for at in range(NZ):
        @pl.when(z == at)
        def _():
            came_plus = [min(at, 8 - p) for p in range(2)]
            on_plus = [0 if at == NZ - 1 else 1 + min(at, 7 - p) for p in range(2)]
            on_minus = [
                sum((at + s) % NZ <= 6 + p for s in range(7 + p)) for p in range(2)
            ]
            wrapped = [
                sum((at + s) % NZ <= 6 + p and at + s >= NZ for s in range(1, 8 + p))
                for p in range(2)
            ]
            sent(0, sum(on_plus))
            sent(1, sum(on_minus))
            passed = sum(came_plus) + sum(wrapped)

            @pl.when(c == 0)
            def _():
                sent(2, passed + 2)

            @pl.when(c == 1)
            def _():
                sent(2, passed)


def call_kernel(*operands):
    vmem = pl.BlockSpec(memory_space=pltpu.VMEM)
    hbm = pl.BlockSpec(memory_space=pl.ANY)
    n = 4 * PAIR
    h = ROWS // 4
    V = lambda *shape: pltpu.VMEM(shape, bf16)
    F = lambda *shape: pltpu.VMEM(shape, f32)
    D = lambda *shape: pltpu.SemaphoreType.DMA(shape)
    return pl.pallas_call(
        layer_kernel,
        out_shape=(
            pltpu.VMEM((ROWS, COLS), bf16),
            pltpu.VMEM((128, COLS), bf16),
        ),
        in_specs=[hbm] * 14,
        out_specs=(vmem, vmem),
        scratch_shapes=[
            V(ROWS, 256), V(ROWS, 256), V(ROWS, 256),
            F(1, 128), F(ROWS, 128), F(ROWS, 128), F(1, 1), F(1, 256), V(128, 2048), F(1, 2048),
            pltpu.VMEM((2, 128), jnp.int32), F(2, 128),
            V(256, ROWS), V(2, ROWS, ROWS), V(2, NZ, PAIR, COLS), V(2, 128, 2 * NZ * PAIR),
            F(2, 128, 128), V(2, 2, ROWS, ROWS),
            V(4 * NZ, ROWS, ROWS),
            pltpu.VMEM((2, ROWS, ROWS), f32),
            pltpu.VMEM((2, 1, ROWS), f32),
            pltpu.VMEM((2, 1, ROWS), f32),
            V(ROWS, 2048), V(2048, 256), V(2048, 256), V(256, 2048),
            V(NZ, PAIR, COLS), V(NZ, PAIR, COLS), V(NZ, PAIR, COLS),
            V(4, 4, 4, 4, PAIR, COLS), V(4, 4, 4, n, COLS), V(4, 3, 4, n, COLS),
            V(4, 4, n, COLS), V(4, 3, n, COLS),
            V(NZ, PAIR, COLS), V(2, NZ, PAIR, COLS),
            V(4, 4, 4, h, COLS), V(4, 3, 4, h, COLS), V(4, 4, h, COLS), V(4, 3, h, COLS),
            D(NZ, 2), D(NZ + 1), D(3), D(2), D(2), D(1), D(1), D(1), D(1), D(4), D(4, 4), D(2), D(2, 4), D(14),
            pltpu.SemaphoreType.REGULAR((2,)),
        ],
        compiler_params=pltpu.CompilerParams(
            collective_id=0, has_side_effects=True, vmem_limit_bytes=60 * 1024 * 1024
        ),
    )(*operands)


def on_device(
    query_maps, key_maps, value_rows, head_lambda, head_gain, out_weight,
    expert_rows, expert_gain, routes, route_weights, gate_weight, up_weight, down_weight,
):
    turns = rope_base ** (-2.0 * (np.arange(128) % 64) / 128)
    return call_kernel(
        query_maps, key_maps, value_rows, jnp.asarray(turns[None], f32),
        head_lambda.reshape(1, 1), head_gain.reshape(1, -1), out_weight, expert_rows,
        expert_gain.reshape(1, -1), routes.T, route_weights.T,
        gate_weight[0], up_weight[0], down_weight[0],
    )


def solution(mesh):
    placed = (
        P("ep", "tp"),
        P("ep", "tp"),
        P("ep", "tp"),
        P("tp"),
        P(),
        P("tp", None),
        P("ep", None),
        P(),
        P("ep", None),
        P("ep", None),
        P("ep", None, "tp"),
        P("ep", None, "tp"),
        P("ep", "tp", None),
    )
    return jax.shard_map(
        on_device,
        mesh=mesh,
        in_specs=placed,
        out_specs=(P("ep", "tp"), P("ep", "tp")),
        check_vma=False,
    )
```

```python
import functools

import jax
import jax.numpy as jnp
import numpy as np
from jax import lax
from jax.experimental import pallas as pl
from jax.experimental.pallas import tpu as pltpu
from jax.sharding import PartitionSpec as P

norm_eps = 1e-06
rope_base = 10000.0
log2e = 1.4426950408889634

NZ = 16
NX = 4
NY = 4
SLOTS = 12
PAIR = 2 * SLOTS
HALF = NZ // 2
ROWS = 256
COLS = 128

MESH = pl.DeviceIdType.MESH
bf16 = jnp.bfloat16
f32 = jnp.float32


def layer_kernel(
    q_hbm, k_hbm, v_hbm, turns_hbm, lam_hbm, gain_hbm, wout_hbm, rows_hbm, rgain_hbm,
    routes_hbm, rweights_hbm, gate_hbm, up_hbm, down_hbm,
    mixed, expert_out,
    q_in, k_in, v_in, turns, cos_t, sin_t, lam, gain, row_in, rgain, routes, rweights,
    q_t, kv_own, disp, pick, spread, weights,
    kv, acc, run_max, run_sum, wout, gate_w, up_w, down_w,
    exch_in, z_send, z_in, ag, rs, rs_in, mid, fin,
    ret_send, ret, tail, tail_in, tail_mid, tail_fin,
    ring_recv, core_recv, kv_sent, pair_send, pair_recv,
    z_sent, z_came, ret_sent, ret_came, plane_send, plane_recv, tail_send, tail_recv, local_sem, known,
):
    ep = lax.axis_index("ep")
    tp = lax.axis_index("tp")
    z = ep // 2
    c = ep % 2
    y = tp // NX
    x = tp % NX
    partner = (z * 2 + 1 - c, tp)
    right = (((z + 1) % NZ) * 2 + c, tp)
    left = (((z + NZ - 1) % NZ) * 2 + c, tp)

    def z_peer(d):
        return (((z + d) % NZ) * 2 + c, tp)

    def x_peer(d):
        return (ep, y * NX + (x + d) % NX)

    def y_peer(d):
        return (ep, ((y + d) % NY) * NX + x)

    def remote(src, dst, send, recv, device):
        return pltpu.make_async_remote_copy(
            src_ref=src, dst_ref=dst, send_sem=send, recv_sem=recv,
            device_id=device, device_id_type=MESH,
        )

    loads = [
        pltpu.make_async_copy(src, dst, local_sem.at[i])
        for i, (src, dst) in enumerate(
            (
                (turns_hbm, turns), (k_hbm, k_in), (v_hbm, v_in),
                (rows_hbm, row_in), (routes_hbm, routes), (rgain_hbm, rgain), (q_hbm, q_in),
                (rweights_hbm, rweights), (gate_hbm, gate_w), (up_hbm, up_w),
                (down_hbm, down_w), (wout_hbm, wout), (gain_hbm, gain), (lam_hbm, lam),
            )
        )
    ]

    barrier = pltpu.get_barrier_semaphore()
    for device in (z_peer(2), z_peer(NZ - 2), right, left, partner):
        pl.semaphore_signal(barrier, inc=1, device_id=device, device_id_type=MESH)
    for d in range(1, 4):
        pl.semaphore_signal(barrier, inc=1, device_id=x_peer(d), device_id_type=MESH)
        pl.semaphore_signal(barrier, inc=1, device_id=y_peer(d), device_id_type=MESH)
    for load in loads:
        load.start()

    def tell(i):
        for d in (2 ** (i + 1), NZ - 2 ** (i + 1)):
            pl.semaphore_signal(known.at[i], inc=1, device_id=z_peer(d), device_id_type=MESH)

    def learn(i):
        pl.semaphore_wait(known.at[i], 2)

    def turned(maps, m):
        wide = maps[:, m * 128:(m + 1) * 128].astype(f32)
        return wide * cos_t[...] + pltpu.roll(wide, 64, 1) * sin_t[...]

    loads[0].wait()
    pl.semaphore_wait(barrier, 5 + 6)
    tell(0)
    lane = lax.broadcasted_iota(jnp.int32, (128, 128), 1)
    spot = lax.broadcasted_iota(jnp.int32, (128, 128), 0) + jnp.where(lane < 64, 0, 128)
    angles = (ep * ROWS + spot).astype(f32) * turns[...]
    for table, packed in ((cos_t, jnp.cos(angles)), (sin_t, jnp.sin(angles))):
        rolled = pltpu.roll(packed, 64, 1)
        low = -1.0 if table is sin_t else 1.0
        table[0:128] = jnp.where(lane < 64, packed * low, rolled)
        table[128:256] = jnp.where(lane < 64, rolled * low, packed)
    loads[1].wait()
    for m in range(2):
        kv_own[0, :, m * 128:(m + 1) * 128] = turned(k_in, m).astype(bf16)
    loads[2].wait()
    kv_own[1] = v_in[...].astype(f32).T.astype(bf16)

    def ring_piece(chip, p):
        return kv.at[chip * 4 + c * 2 + p]

    def ring_wait(chip, p):
        here = ring_piece(chip, p)
        remote(here, here, kv_sent.at[0], ring_recv.at[chip, p], left).wait_recv()

    def core_wait(chip):
        here = kv.at[pl.ds(chip * 4 + 2 - c * 2, 2)]
        remote(here, here, kv_sent.at[2], core_recv.at[chip], partner).wait_recv()

    def core_wait_one(chip, p, mark):
        here = kv.at[chip * 4 + 2 - c * 2 + p]
        remote(here, here, kv_sent.at[2], core_recv.at[mark], partner).wait_recv()

    def ring_copy(src, chip, p, way, device):
        return remote(src, ring_piece(chip, p), kv_sent.at[way], ring_recv.at[chip, p], device)

    def core_copy(src, chip, p, mark):
        return remote(src, ring_piece(chip, p), kv_sent.at[2], core_recv.at[mark], partner)

    def send_own(p):
        @pl.when(z < NZ - 1)
        def _():
            ring_copy(kv_own.at[p], z, p, 0, right).start()

        @pl.when(z <= 7 - p)
        def _():
            ring_copy(kv_own.at[1 - p], z, 1 - p, 1, left).start()

        @pl.when(c == 0)
        def _():
            core_copy(kv_own.at[p], z, p, z).start()

    send_own(0)
    send_own(1)

    for i in range(3, 6):
        loads[i].wait()
    wide = row_in[...].astype(f32)
    level = lax.rsqrt(jnp.mean(wide * wide, axis=1, keepdims=True) + norm_eps)
    column = pl.ds(pl.multiple_of(tp * COLS, COLS), COLS)
    normed = (row_in[:, column].astype(f32) * level * rgain[:, column]).astype(bf16)
    chosen = [routes[k:k + 1, :] for k in range(2)]
    names = lax.broadcasted_iota(jnp.int32, (32, 128), 0)
    hot = [(names == r).astype(f32) for r in chosen]
    earlier = (
        lax.broadcasted_iota(jnp.int32, (128, 128), 0)
        < lax.broadcasted_iota(jnp.int32, (128, 128), 1)
    )
    counts = jnp.dot(
        (hot[0] + hot[1]).astype(bf16), earlier.astype(f32).astype(bf16),
        preferred_element_type=f32,
    )
    lines = lax.broadcasted_iota(jnp.int32, (2 * NZ * PAIR, 128), 0).astype(f32)
    base = [
        ((r // 2) * PAIR + c * SLOTS).astype(f32) + jnp.sum(counts * h, axis=0, keepdims=True)
        for r, h in zip(chosen, hot)
    ]
    block = float(NZ * PAIR)
    to_row = [b + (r % 2).astype(f32) * block for b, r in zip(base, chosen)]
    from_row = [
        b + jnp.where(r % 2 == c, 0.0, block) for b, r in zip(base, chosen)
    ]
    spot_of = jnp.where((lines == to_row[0]) | (lines == to_row[1]), 1.0, 0.0).astype(bf16)
    disp[...] = (
        jnp.dot(spot_of, normed, preferred_element_type=f32)
        .astype(bf16)
        .reshape(2, NZ, PAIR, COLS)
    )
    exch = remote(disp.at[1 - c], exch_in, pair_send.at[0], pair_recv.at[0], partner)
    exch.start()
    learn(0)
    tell(1)

    loads[6].wait()
    for m in range(2):
        q_t[m * 128:(m + 1) * 128, :] = turned(q_in, m).T.astype(bf16)
    exch.wait_recv()
    z_send[...] = (disp[c].astype(f32) + exch_in[...].astype(f32)).astype(bf16)
    z_in[z] = z_send[z]

    def dispatch():
        learn(1)
        for d in range(1, NZ):
            remote(
                z_send.at[(z + d) % NZ], z_in.at[z], z_sent.at[0], z_came.at[0], z_peer(d)
            ).start()

    loads[7].wait()
    for k in range(2):
        pick[k] = jnp.where(lines == from_row[k], 1.0, 0.0).T.astype(bf16)
        spread[k] = jnp.broadcast_to(rweights[k:k + 1, :], (128, 128)).T

    scale = (128 ** -0.5) * log2e

    def fold(k_of, v_of, count, masked, first, later=False):
        for m in range(2):
            q_m = q_t[m * 128:(m + 1) * 128, :]
            scores = []
            for i in range(count):
                s = jnp.dot(k_of(i)[:, m * 128:(m + 1) * 128], q_m, preferred_element_type=f32)
                if masked:
                    rows = lax.broadcasted_iota(jnp.int32, s.shape, 0)
                    cols = lax.broadcasted_iota(jnp.int32, s.shape, 1)
                    s = jnp.where(rows <= cols, s, -1e30)
                scores.append(s)
            top = jnp.max(scores[0], axis=0, keepdims=True)
            for s in scores[1:]:
                top = jnp.maximum(top, jnp.max(s, axis=0, keepdims=True))
            top = top * scale
            if first:
                new_max = top
            else:
                old = run_max[m]
                new_max = jnp.maximum(old, top)
                alpha = jnp.exp2(old - new_max)
            total = None
            out = None
            for i in range(count):
                e = jnp.exp2(scores[i] * scale - new_max)
                t = jnp.sum(e, axis=0, keepdims=True)
                total = t if total is None else total + t
                if later:
                    weights[m, i] = e.astype(bf16)
                else:
                    o = jnp.dot(v_of(i), e.astype(bf16), preferred_element_type=f32)
                    out = o if out is None else out + o
            run_max[m] = new_max
            if first:
                run_sum[m] = total
                acc[m] = out
            else:
                run_sum[m] = run_sum[m] * alpha + total
                acc[m] = acc[m] * alpha if later else acc[m] * alpha + out

    fold(lambda i: kv_own[0], lambda i: kv_own[1], 1, True, True)

    @pl.when(c == 1)
    def _():
        core_wait(z)
        fold(lambda i: kv[z * 4], lambda i: kv[z * 4 + 1], 1, False, False)

    def fold_chip(chip):
        core_wait(chip)
        fold(
            lambda i: kv[chip * 4 + i * 2], lambda i: kv[chip * 4 + i * 2 + 1], 2, False, False
        )

    place = [(y, x), (x, y)]
    first_peer = (x_peer, y_peer)
    second_peer = (y_peer, x_peer)

    def group_send(phase, g, src_of, dst_of, peer):
        for d in range(1, 4):
            remote(
                src_of(d), dst_of(d), plane_send.at[phase], plane_recv.at[phase, g], peer(d)
            ).start()

    def group_three(phase, g, ref):
        return remote(ref, ref, plane_send.at[phase], plane_recv.at[phase, g], partner)

    def tail_group(phase, g, src_of, dst_of, peer):
        for d in range(1, 4):
            remote(
                src_of(d), dst_of(d), tail_send.at[phase], tail_recv.at[phase, g], peer(d)
            ).start()

    def tail_three(phase, g, ref):
        return remote(ref, ref, tail_send.at[phase], tail_recv.at[phase, g], partner)

    few = pl.ds(0, 3)

    def gather_one():
        most = pl.ds(0, NZ - 1)
        remote(
            z_send.at[most], z_in.at[most], z_sent.at[0], z_came.at[0], partner
        ).wait_recv()
        for g in range(4):
            u, v = place[g % 2]
            block = pl.ds(4 * g, 4)
            ag[g, u, v] = z_in[block]
            group_send(
                0, g, lambda d: z_in.at[block], lambda d: ag.at[g, u, v], first_peer[g % 2]
            )

    def gather_two():
        for g in range(4):
            u, v = place[g % 2]
            group_three(0, g, ag.at[g, 0, few]).wait_recv()
            group_send(
                1, g, lambda d: ag.at[g, u], lambda d: ag.at[g, u], second_peer[g % 2]
            )

    n = 4 * PAIR

    def expert(r):
        if r == 0:
            for load in loads[8:11]:
                load.wait()
        for g in (2 * r, 2 * r + 1):
            group_three(1, g, ag.at[g, few]).wait_recv()
        pieces = [
            jnp.concatenate(
                [ag[2 * r, i, j].reshape(n, COLS), ag[2 * r + 1, j, i].reshape(n, COLS)], axis=0
            )
            for i in range(NY)
            for j in range(NX)
        ]
        rows = jnp.concatenate(pieces, axis=1)
        gates = jnp.dot(rows, gate_w[...], preferred_element_type=f32)
        ups = jnp.dot(rows, up_w[...], preferred_element_type=f32)
        hidden = (gates / (1.0 + jnp.exp(-gates)) * ups).astype(bf16)
        for i in range(NY):
            for j in range(NX):
                at = (i * NX + j) * COLS
                part = jnp.dot(
                    hidden, down_w[:, at:at + COLS], preferred_element_type=f32
                ).astype(bf16)
                rs[2 * r, i, j] = part[:n]
                rs[2 * r + 1, j, i] = part[n:]
        for g in (2 * r, 2 * r + 1):
            u, v = place[g % 2]
            group_send(
                2, g, lambda d: rs.at[g, (u + d) % 4], lambda d: rs_in.at[g, d - 1],
                second_peer[g % 2],
            )

    def sum_one(r):
        for g in (2 * r, 2 * r + 1):
            u, v = place[g % 2]
            group_three(2, g, rs_in.at[g]).wait_recv()
            for j in range(4):
                t = rs[g, u, j].astype(f32)
                for d in range(3):
                    t = t + rs_in[g, d, j].astype(f32)
                mid[g, j] = t.astype(bf16)
            group_send(
                3, g, lambda d: mid.at[g, (v + d) % 4], lambda d: fin.at[g, d - 1],
                first_peer[g % 2],
            )

    def sum_two(g):
        u, v = place[g % 2]
        group_three(3, g, fin.at[g]).wait_recv()
        t = mid[g, v].astype(f32)
        for d in range(3):
            t = t + fin[g, d].astype(f32)
        ret_send[4 * g:4 * g + 4] = t.astype(bf16).reshape(4, PAIR, COLS)
        for to in range(4 * g, 4 * g + 4):
            @pl.when(z == to)
            def _():
                ret[0, to] = ret_send[to]

            @pl.when(z != to)
            def _():
                remote(
                    ret_send.at[to], ret.at[0, z], ret_sent.at[0], ret_came.at[0],
                    (to * 2 + c, tp),
                ).start()

    def tick(s, carry):
        zl = jnp.maximum(z - s, 0)
        zr = (z + s) % NZ
        wrapped = z + s >= NZ

        def plus(p, last):
            @pl.when((s <= last) & (s <= z))
            def _():
                ring_wait(zl, p)

                @pl.when((z < NZ - 1) & (s < last))
                def _():
                    ring_copy(ring_piece(zl, p), zl, p, 0, right).start()

                core_copy(ring_piece(zl, p), zl, p, zl).start()

        def minus(p, last):
            @pl.when((s <= last) & (zr <= 6 + p))
            def _():
                ring_wait(zr, p)

                @pl.when(s < last)
                def _():
                    ring_copy(ring_piece(zr, p), zr, p, 1, left).start()

                @pl.when(wrapped)
                def _():
                    mark = jnp.where(s == 8, NZ, zr)
                    core_copy(ring_piece(zr, p), zr, p, mark).start()

        def fold_minus():
            @pl.when((s >= 2) & (s - 1 <= 7) & (z + s - 1 >= NZ))
            def _():
                fold_chip(jnp.maximum(z + s - 1 - NZ, 0))

        @pl.when(s == 5)
        def _():
            expert(0)

        def fold_plus():
            @pl.when((s >= 2) & (s - 1 <= z))
            def _():
                fold_chip(jnp.maximum(z - s + 1, 0))

        @pl.when((s == 8) & (c == 0))
        def _():
            fold_plus()
            fold_minus()

        plus(0, 8)
        minus(1, 8)

        @pl.when(s == 1)
        def _():
            dispatch()

        @pl.when(s == 7)
        def _():
            sum_one(1)

        @pl.when((s == 7) & (z >= 8))
        def _():
            sum_two(0)

        @pl.when((s < 8) | (c == 1))
        def _():
            fold_plus()

        @pl.when((s == 8) & (c == 1))
        def _():
            fold_minus()

        @pl.when(s == 6)
        def _():
            sum_one(0)

        @pl.when((s == 8) & (z >= 8))
        def _():
            far = jnp.maximum(z - 8, 0)
            core_wait_one(far, 0, far)
            fold(lambda i: kv[far * 4 + i * 2], None, 2, False, False, later=True)

        plus(1, 7)
        minus(0, 7)

        @pl.when(s == 2)
        def _():
            gather_one()

        @pl.when(s == 3)
        def _():
            gather_two()

        @pl.when(s == 5)
        def _():
            expert(1)

        @pl.when(s < 8)
        def _():
            fold_minus()

        return carry

    lax.fori_loop(1, 9, tick, 0)

    @pl.when(z >= 8)
    def _():
        sum_two(1)
        sum_two(2)
        sum_two(3)
        far = jnp.maximum(z - 8, 0)
        core_wait_one(far, 1, NZ)
        for m in range(2):
            out = jnp.dot(kv[far * 4 + 1], weights[m, 0], preferred_element_type=f32)
            acc[m] = acc[m] + (
                out + jnp.dot(kv[far * 4 + 3], weights[m, 1], preferred_element_type=f32)
            )


    @pl.when(z < 8)
    def _():
        sum_two(0)
        sum_two(1)

    for load in loads[11:14]:
        load.wait()
    first = acc[0] / run_sum[0]
    second = acc[1] / run_sum[1]
    diff = first - lam[...] * second
    mean = jnp.mean(diff * diff, axis=0, keepdims=True)
    head_t = diff * lax.rsqrt(mean + norm_eps)
    for half in range(2):
        head = (head_t[:, half * 128:(half + 1) * 128].T * gain[...]).astype(bf16)
        for i in range(NY):
            for j in range(NX):
                at = (i * NX + j) * COLS
                part = jnp.dot(
                    head, wout[:, at:at + COLS], preferred_element_type=f32
                ).astype(bf16)
                tail[2 * half, i, j] = part[:64]
                tail[2 * half + 1, j, i] = part[64:]
        for g in (2 * half, 2 * half + 1):
            u, v = place[g % 2]
            tail_group(
                0, g, lambda d: tail.at[g, (u + d) % 4], lambda d: tail_in.at[g, d - 1],
                second_peer[g % 2],
            )

    for g in range(4):
        u, v = place[g % 2]
        tail_three(0, g, tail_in.at[g]).wait_recv()
        for j in range(4):
            t = tail[g, u, j].astype(f32)
            for d in range(3):
                t = t + tail_in[g, d, j].astype(f32)
            tail_mid[g, j] = t.astype(bf16)
        tail_group(
            1, g, lambda d: tail_mid.at[g, (v + d) % 4], lambda d: tail_fin.at[g, d - 1],
            first_peer[g % 2],
        )
        if g == 1:
            @pl.when(z < 8)
            def _():
                sum_two(2)
                sum_two(3)

    most = pl.ds(0, NZ - 1)
    remote(
        ret_send.at[most], ret.at[0, most], ret_sent.at[0], ret_came.at[0], partner
    ).wait_recv()
    back = remote(ret.at[0], ret.at[1], pair_send.at[1], pair_recv.at[1], partner)
    back.start()

    back.wait_recv()
    rows = ret[...].reshape(2 * NZ * PAIR, COLS)
    mixture = jnp.dot(pick[0], rows, preferred_element_type=f32) * spread[0]
    mixture = mixture + jnp.dot(pick[1], rows, preferred_element_type=f32) * spread[1]
    expert_out[...] = mixture.astype(bf16)

    for g in range(4):
        tail_three(1, g, tail_fin.at[g]).wait_recv()
        t = tail_mid[g, place[g % 2][1]].astype(f32)
        for d in range(3):
            t = t + tail_fin[g, d].astype(f32)
        mixed[64 * g:64 * (g + 1)] = t.astype(bf16)

    exch.wait_send()
    back.wait_send()
    remote(z_send.at[most], z_in.at[most], z_sent.at[0], z_came.at[0], partner).wait_send()
    remote(
        ret_send.at[most], ret.at[0, most], ret_sent.at[0], ret_came.at[0], partner
    ).wait_send()
    group_three(0, 0, ag.at[0, few]).wait_send()
    group_three(1, 0, ag.at[few]).wait_send()
    group_three(2, 0, rs_in).wait_send()
    group_three(3, 0, fin).wait_send()
    tail_three(0, 0, tail_in).wait_send()
    tail_three(1, 0, tail_fin).wait_send()

    def sent(way, count):
        if count:
            here = kv.at[pl.ds(0, count)]
            remote(here, here, kv_sent.at[way], core_recv.at[0], partner).wait_send()

    for at in range(NZ):
        @pl.when(z == at)
        def _():
            came_plus = [min(at, 8 - p) for p in range(2)]
            on_plus = [0 if at == NZ - 1 else 1 + min(at, 7 - p) for p in range(2)]
            on_minus = [
                sum((at + s) % NZ <= 6 + p for s in range(7 + p)) for p in range(2)
            ]
            wrapped = [
                sum((at + s) % NZ <= 6 + p and at + s >= NZ for s in range(1, 8 + p))
                for p in range(2)
            ]
            sent(0, sum(on_plus))
            sent(1, sum(on_minus))
            passed = sum(came_plus) + sum(wrapped)

            @pl.when(c == 0)
            def _():
                sent(2, passed + 2)

            @pl.when(c == 1)
            def _():
                sent(2, passed)


def call_kernel(*operands):
    vmem = pl.BlockSpec(memory_space=pltpu.VMEM)
    hbm = pl.BlockSpec(memory_space=pl.ANY)
    n = 4 * PAIR
    h = ROWS // 4
    V = lambda *shape: pltpu.VMEM(shape, bf16)
    F = lambda *shape: pltpu.VMEM(shape, f32)
    D = lambda *shape: pltpu.SemaphoreType.DMA(shape)
    return pl.pallas_call(
        layer_kernel,
        out_shape=(
            pltpu.VMEM((ROWS, COLS), bf16),
            pltpu.VMEM((128, COLS), bf16),
        ),
        in_specs=[hbm] * 14,
        out_specs=(vmem, vmem),
        scratch_shapes=[
            V(ROWS, 256), V(ROWS, 256), V(ROWS, 256),
            F(1, 128), F(ROWS, 128), F(ROWS, 128), F(1, 1), F(1, 256), V(128, 2048), F(1, 2048),
            pltpu.VMEM((2, 128), jnp.int32), F(2, 128),
            V(256, ROWS), V(2, ROWS, ROWS), V(2, NZ, PAIR, COLS), V(2, 128, 2 * NZ * PAIR),
            F(2, 128, 128), V(2, 2, ROWS, ROWS),
            V(4 * NZ, ROWS, ROWS),
            pltpu.VMEM((2, ROWS, ROWS), f32),
            pltpu.VMEM((2, 1, ROWS), f32),
            pltpu.VMEM((2, 1, ROWS), f32),
            V(ROWS, 2048), V(2048, 256), V(2048, 256), V(256, 2048),
            V(NZ, PAIR, COLS), V(NZ, PAIR, COLS), V(NZ, PAIR, COLS),
            V(4, 4, 4, 4, PAIR, COLS), V(4, 4, 4, n, COLS), V(4, 3, 4, n, COLS),
            V(4, 4, n, COLS), V(4, 3, n, COLS),
            V(NZ, PAIR, COLS), V(2, NZ, PAIR, COLS),
            V(4, 4, 4, h, COLS), V(4, 3, 4, h, COLS), V(4, 4, h, COLS), V(4, 3, h, COLS),
            D(NZ, 2), D(NZ + 1), D(3), D(2), D(2), D(1), D(1), D(1), D(1), D(4), D(4, 4), D(2), D(2, 4), D(14),
            pltpu.SemaphoreType.REGULAR((2,)),
        ],
        compiler_params=pltpu.CompilerParams(
            collective_id=0, has_side_effects=True, vmem_limit_bytes=60 * 1024 * 1024
        ),
    )(*operands)


def on_device(
    query_maps, key_maps, value_rows, head_lambda, head_gain, out_weight,
    expert_rows, expert_gain, routes, route_weights, gate_weight, up_weight, down_weight,
):
    turns = rope_base ** (-2.0 * (np.arange(128) % 64) / 128)
    return call_kernel(
        query_maps, key_maps, value_rows, jnp.asarray(turns[None], f32),
        head_lambda.reshape(1, 1), head_gain.reshape(1, -1), out_weight, expert_rows,
        expert_gain.reshape(1, -1), routes.T, route_weights.T,
        gate_weight[0], up_weight[0], down_weight[0],
    )


def solution(mesh):
    placed = (
        P("ep", "tp"),
        P("ep", "tp"),
        P("ep", "tp"),
        P("tp"),
        P(),
        P("tp", None),
        P("ep", None),
        P(),
        P("ep", None),
        P("ep", None),
        P("ep", None, "tp"),
        P("ep", None, "tp"),
        P("ep", "tp", None),
    )
    return jax.shard_map(
        on_device,
        mesh=mesh,
        in_specs=placed,
        out_specs=(P("ep", "tp"), P("ep", "tp")),
        check_vma=False,
    )
```

```python
import functools

import jax
import jax.numpy as jnp
import numpy as np
from jax import lax
from jax.experimental import pallas as pl
from jax.experimental.pallas import tpu as pltpu
from jax.sharding import PartitionSpec as P

norm_eps = 1e-06
rope_base = 10000.0
log2e = 1.4426950408889634

NZ = 16
NX = 4
NY = 4
SLOTS = 12
PAIR = 2 * SLOTS
HALF = NZ // 2
ROWS = 256
COLS = 128

MESH = pl.DeviceIdType.MESH
bf16 = jnp.bfloat16
f32 = jnp.float32


def layer_kernel(
    q_hbm, k_hbm, v_hbm, turns_hbm, lam_hbm, gain_hbm, wout_hbm, rows_hbm, rgain_hbm,
    routes_hbm, rweights_hbm, gate_hbm, up_hbm, down_hbm,
    mixed, expert_out,
    q_in, k_in, v_in, turns, cos_t, sin_t, lam, gain, row_in, rgain, routes, rweights,
    q_t, kv_own, disp, pick, spread, weights,
    kv, acc, run_max, run_sum, wout, gate_w, up_w, down_w,
    exch_in, z_send, z_in, ag, rs, rs_in, mid, fin,
    ret_send, ret, tail, tail_in, tail_mid, tail_fin,
    ring_recv, core_recv, kv_sent, pair_send, pair_recv,
    z_sent, z_came, ret_sent, ret_came, plane_send, plane_recv, tail_send, tail_recv, local_sem, known,
):
    ep = lax.axis_index("ep")
    tp = lax.axis_index("tp")
    z = ep // 2
    c = ep % 2
    y = tp // NX
    x = tp % NX
    partner = (z * 2 + 1 - c, tp)
    right = (((z + 1) % NZ) * 2 + c, tp)
    left = (((z + NZ - 1) % NZ) * 2 + c, tp)

    def z_peer(d):
        return (((z + d) % NZ) * 2 + c, tp)

    def x_peer(d):
        return (ep, y * NX + (x + d) % NX)

    def y_peer(d):
        return (ep, ((y + d) % NY) * NX + x)

    def remote(src, dst, send, recv, device):
        return pltpu.make_async_remote_copy(
            src_ref=src, dst_ref=dst, send_sem=send, recv_sem=recv,
            device_id=device, device_id_type=MESH,
        )

    loads = [
        pltpu.make_async_copy(src, dst, local_sem.at[i])
        for i, (src, dst) in enumerate(
            (
                (turns_hbm, turns), (k_hbm, k_in), (v_hbm, v_in),
                (rows_hbm, row_in), (routes_hbm, routes), (rgain_hbm, rgain), (q_hbm, q_in),
                (rweights_hbm, rweights), (gate_hbm, gate_w), (up_hbm, up_w),
                (down_hbm, down_w), (wout_hbm, wout), (gain_hbm, gain), (lam_hbm, lam),
            )
        )
    ]

    for load in loads[:3]:
        load.start()
    barrier = pltpu.get_barrier_semaphore()
    for device in (z_peer(2), z_peer(NZ - 2), right, left, partner):
        pl.semaphore_signal(barrier, inc=1, device_id=device, device_id_type=MESH)
    for d in range(1, 4):
        pl.semaphore_signal(barrier, inc=1, device_id=x_peer(d), device_id_type=MESH)
        pl.semaphore_signal(barrier, inc=1, device_id=y_peer(d), device_id_type=MESH)
    for load in loads[3:]:
        load.start()

    def tell(i):
        for d in (2 ** (i + 1), NZ - 2 ** (i + 1)):
            pl.semaphore_signal(known.at[i], inc=1, device_id=z_peer(d), device_id_type=MESH)

    def learn(i):
        pl.semaphore_wait(known.at[i], 2)

    def turned(maps, m):
        wide = maps[:, m * 128:(m + 1) * 128].astype(f32)
        return wide * cos_t[...] + pltpu.roll(wide, 64, 1) * sin_t[...]

    loads[0].wait()
    pl.semaphore_wait(barrier, 5 + 6)
    tell(0)
    lane = lax.broadcasted_iota(jnp.int32, (128, 128), 1)
    spot = lax.broadcasted_iota(jnp.int32, (128, 128), 0) + jnp.where(lane < 64, 0, 128)
    angles = (ep * ROWS + spot).astype(f32) * turns[...]
    for table, packed in ((cos_t, jnp.cos(angles)), (sin_t, jnp.sin(angles))):
        rolled = pltpu.roll(packed, 64, 1)
        low = -1.0 if table is sin_t else 1.0
        table[0:128] = jnp.where(lane < 64, packed * low, rolled)
        table[128:256] = jnp.where(lane < 64, rolled * low, packed)
    loads[1].wait()
    for m in range(2):
        kv_own[0, :, m * 128:(m + 1) * 128] = turned(k_in, m).astype(bf16)
    loads[2].wait()
    kv_own[1] = v_in[...].astype(f32).T.astype(bf16)

    def ring_piece(chip, p):
        return kv.at[chip * 4 + c * 2 + p]

    def ring_wait(chip, p):
        here = ring_piece(chip, p)
        remote(here, here, kv_sent.at[0], ring_recv.at[chip, p], left).wait_recv()

    def core_wait(chip):
        here = kv.at[pl.ds(chip * 4 + 2 - c * 2, 2)]
        remote(here, here, kv_sent.at[2], core_recv.at[chip], partner).wait_recv()

    def core_wait_one(chip, p, mark):
        here = kv.at[chip * 4 + 2 - c * 2 + p]
        remote(here, here, kv_sent.at[2], core_recv.at[mark], partner).wait_recv()

    def ring_copy(src, chip, p, way, device):
        return remote(src, ring_piece(chip, p), kv_sent.at[way], ring_recv.at[chip, p], device)

    def core_copy(src, chip, p, mark):
        return remote(src, ring_piece(chip, p), kv_sent.at[2], core_recv.at[mark], partner)

    def send_own(p):
        @pl.when(z < NZ - 1)
        def _():
            ring_copy(kv_own.at[p], z, p, 0, right).start()

        @pl.when(z <= 7 - p)
        def _():
            ring_copy(kv_own.at[1 - p], z, 1 - p, 1, left).start()

        @pl.when(c == 0)
        def _():
            core_copy(kv_own.at[p], z, p, z).start()

    send_own(0)
    send_own(1)

    for i in range(3, 6):
        loads[i].wait()
    wide = row_in[...].astype(f32)
    level = lax.rsqrt(jnp.mean(wide * wide, axis=1, keepdims=True) + norm_eps)
    column = pl.ds(pl.multiple_of(tp * COLS, COLS), COLS)
    normed = (row_in[:, column].astype(f32) * level * rgain[:, column]).astype(bf16)
    chosen = [routes[k:k + 1, :] for k in range(2)]
    names = lax.broadcasted_iota(jnp.int32, (32, 128), 0)
    hot = [(names == r).astype(f32) for r in chosen]
    earlier = (
        lax.broadcasted_iota(jnp.int32, (128, 128), 0)
        < lax.broadcasted_iota(jnp.int32, (128, 128), 1)
    )
    counts = jnp.dot(
        (hot[0] + hot[1]).astype(bf16), earlier.astype(f32).astype(bf16),
        preferred_element_type=f32,
    )
    lines = lax.broadcasted_iota(jnp.int32, (2 * NZ * PAIR, 128), 0).astype(f32)
    base = [
        ((r // 2) * PAIR + c * SLOTS).astype(f32) + jnp.sum(counts * h, axis=0, keepdims=True)
        for r, h in zip(chosen, hot)
    ]
    block = float(NZ * PAIR)
    to_row = [b + (r % 2).astype(f32) * block for b, r in zip(base, chosen)]
    from_row = [
        b + jnp.where(r % 2 == c, 0.0, block) for b, r in zip(base, chosen)
    ]
    spot_of = jnp.where((lines == to_row[0]) | (lines == to_row[1]), 1.0, 0.0).astype(bf16)
    disp[...] = (
        jnp.dot(spot_of, normed, preferred_element_type=f32)
        .astype(bf16)
        .reshape(2, NZ, PAIR, COLS)
    )
    exch = remote(disp.at[1 - c], exch_in, pair_send.at[0], pair_recv.at[0], partner)
    exch.start()
    learn(0)
    tell(1)

    loads[6].wait()
    for m in range(2):
        q_t[m * 128:(m + 1) * 128, :] = turned(q_in, m).T.astype(bf16)
    exch.wait_recv()
    z_send[...] = (disp[c].astype(f32) + exch_in[...].astype(f32)).astype(bf16)
    z_in[z] = z_send[z]

    def dispatch():
        learn(1)
        for d in range(1, NZ):
            remote(
                z_send.at[(z + d) % NZ], z_in.at[z], z_sent.at[0], z_came.at[0], z_peer(d)
            ).start()

    loads[7].wait()
    for k in range(2):
        pick[k] = jnp.where(lines == from_row[k], 1.0, 0.0).T.astype(bf16)
        spread[k] = jnp.broadcast_to(rweights[k:k + 1, :], (128, 128)).T

    scale = (128 ** -0.5) * log2e

    def fold(k_of, v_of, count, masked, first, later=False):
        for m in range(2):
            q_m = q_t[m * 128:(m + 1) * 128, :]
            scores = []
            for i in range(count):
                s = jnp.dot(k_of(i)[:, m * 128:(m + 1) * 128], q_m, preferred_element_type=f32)
                if masked:
                    rows = lax.broadcasted_iota(jnp.int32, s.shape, 0)
                    cols = lax.broadcasted_iota(jnp.int32, s.shape, 1)
                    s = jnp.where(rows <= cols, s, -1e30)
                scores.append(s)
            top = jnp.max(scores[0], axis=0, keepdims=True)
            for s in scores[1:]:
                top = jnp.maximum(top, jnp.max(s, axis=0, keepdims=True))
            top = top * scale
            if first:
                new_max = top
            else:
                old = run_max[m]
                new_max = jnp.maximum(old, top)
                alpha = jnp.exp2(old - new_max)
            total = None
            out = None
            for i in range(count):
                e = jnp.exp2(scores[i] * scale - new_max)
                t = jnp.sum(e, axis=0, keepdims=True)
                total = t if total is None else total + t
                if later:
                    weights[m, i] = e.astype(bf16)
                else:
                    o = jnp.dot(v_of(i), e.astype(bf16), preferred_element_type=f32)
                    out = o if out is None else out + o
            run_max[m] = new_max
            if first:
                run_sum[m] = total
                acc[m] = out
            else:
                run_sum[m] = run_sum[m] * alpha + total
                acc[m] = acc[m] * alpha if later else acc[m] * alpha + out

    fold(lambda i: kv_own[0], lambda i: kv_own[1], 1, True, True)

    @pl.when(c == 1)
    def _():
        core_wait(z)
        fold(lambda i: kv[z * 4], lambda i: kv[z * 4 + 1], 1, False, False)

    def fold_chip(chip):
        core_wait(chip)
        fold(
            lambda i: kv[chip * 4 + i * 2], lambda i: kv[chip * 4 + i * 2 + 1], 2, False, False
        )

    place = [(y, x), (x, y)]
    first_peer = (x_peer, y_peer)
    second_peer = (y_peer, x_peer)

    def group_send(phase, g, src_of, dst_of, peer):
        for d in range(1, 4):
            remote(
                src_of(d), dst_of(d), plane_send.at[phase], plane_recv.at[phase, g], peer(d)
            ).start()

    def group_three(phase, g, ref):
        return remote(ref, ref, plane_send.at[phase], plane_recv.at[phase, g], partner)

    def tail_group(phase, g, src_of, dst_of, peer):
        for d in range(1, 4):
            remote(
                src_of(d), dst_of(d), tail_send.at[phase], tail_recv.at[phase, g], peer(d)
            ).start()

    def tail_three(phase, g, ref):
        return remote(ref, ref, tail_send.at[phase], tail_recv.at[phase, g], partner)

    few = pl.ds(0, 3)

    def gather_one():
        most = pl.ds(0, NZ - 1)
        remote(
            z_send.at[most], z_in.at[most], z_sent.at[0], z_came.at[0], partner
        ).wait_recv()
        for g in range(4):
            u, v = place[g % 2]
            block = pl.ds(4 * g, 4)
            ag[g, u, v] = z_in[block]
            group_send(
                0, g, lambda d: z_in.at[block], lambda d: ag.at[g, u, v], first_peer[g % 2]
            )

    def gather_two():
        for g in range(4):
            u, v = place[g % 2]
            group_three(0, g, ag.at[g, 0, few]).wait_recv()
            group_send(
                1, g, lambda d: ag.at[g, u], lambda d: ag.at[g, u], second_peer[g % 2]
            )

    n = 4 * PAIR

    def expert(r):
        if r == 0:
            for load in loads[8:11]:
                load.wait()
        for g in (2 * r, 2 * r + 1):
            group_three(1, g, ag.at[g, few]).wait_recv()
        pieces = [
            jnp.concatenate(
                [ag[2 * r, i, j].reshape(n, COLS), ag[2 * r + 1, j, i].reshape(n, COLS)], axis=0
            )
            for i in range(NY)
            for j in range(NX)
        ]
        rows = jnp.concatenate(pieces, axis=1)
        gates = jnp.dot(rows, gate_w[...], preferred_element_type=f32)
        ups = jnp.dot(rows, up_w[...], preferred_element_type=f32)
        hidden = (gates / (1.0 + jnp.exp(-gates)) * ups).astype(bf16)
        for i in range(NY):
            for j in range(NX):
                at = (i * NX + j) * COLS
                part = jnp.dot(
                    hidden, down_w[:, at:at + COLS], preferred_element_type=f32
                ).astype(bf16)
                rs[2 * r, i, j] = part[:n]
                rs[2 * r + 1, j, i] = part[n:]
        for g in (2 * r, 2 * r + 1):
            u, v = place[g % 2]
            group_send(
                2, g, lambda d: rs.at[g, (u + d) % 4], lambda d: rs_in.at[g, d - 1],
                second_peer[g % 2],
            )

    def sum_one(r):
        for g in (2 * r, 2 * r + 1):
            u, v = place[g % 2]
            group_three(2, g, rs_in.at[g]).wait_recv()
            for j in range(4):
                t = rs[g, u, j].astype(f32)
                for d in range(3):
                    t = t + rs_in[g, d, j].astype(f32)
                mid[g, j] = t.astype(bf16)
            group_send(
                3, g, lambda d: mid.at[g, (v + d) % 4], lambda d: fin.at[g, d - 1],
                first_peer[g % 2],
            )

    def sum_two(g):
        u, v = place[g % 2]
        group_three(3, g, fin.at[g]).wait_recv()
        t = mid[g, v].astype(f32)
        for d in range(3):
            t = t + fin[g, d].astype(f32)
        ret_send[4 * g:4 * g + 4] = t.astype(bf16).reshape(4, PAIR, COLS)
        for to in range(4 * g, 4 * g + 4):
            @pl.when(z == to)
            def _():
                ret[0, to] = ret_send[to]

            @pl.when(z != to)
            def _():
                remote(
                    ret_send.at[to], ret.at[0, z], ret_sent.at[0], ret_came.at[0],
                    (to * 2 + c, tp),
                ).start()

    def tick(s, carry):
        zl = jnp.maximum(z - s, 0)
        zr = (z + s) % NZ
        wrapped = z + s >= NZ

        def plus(p, last):
            @pl.when((s <= last) & (s <= z))
            def _():
                ring_wait(zl, p)

                @pl.when((z < NZ - 1) & (s < last))
                def _():
                    ring_copy(ring_piece(zl, p), zl, p, 0, right).start()

                core_copy(ring_piece(zl, p), zl, p, zl).start()

        def minus(p, last):
            @pl.when((s <= last) & (zr <= 6 + p))
            def _():
                ring_wait(zr, p)

                @pl.when(s < last)
                def _():
                    ring_copy(ring_piece(zr, p), zr, p, 1, left).start()

                @pl.when(wrapped)
                def _():
                    mark = jnp.where(s == 8, NZ, zr)
                    core_copy(ring_piece(zr, p), zr, p, mark).start()

        def fold_minus():
            @pl.when((s >= 2) & (s - 1 <= 7) & (z + s - 1 >= NZ))
            def _():
                fold_chip(jnp.maximum(z + s - 1 - NZ, 0))

        @pl.when(s == 5)
        def _():
            expert(0)

        def fold_plus():
            @pl.when((s >= 2) & (s - 1 <= z))
            def _():
                fold_chip(jnp.maximum(z - s + 1, 0))

        @pl.when((s == 8) & (c == 0))
        def _():
            fold_plus()
            fold_minus()

        plus(0, 8)
        minus(1, 8)

        @pl.when(s == 1)
        def _():
            dispatch()

        @pl.when(s == 7)
        def _():
            sum_one(1)

        @pl.when((s == 7) & (z >= 8))
        def _():
            sum_two(0)

        @pl.when((s < 8) | (c == 1))
        def _():
            fold_plus()

        @pl.when((s == 8) & (c == 1))
        def _():
            fold_minus()

        @pl.when(s == 6)
        def _():
            sum_one(0)

        @pl.when((s == 8) & (z >= 8))
        def _():
            far = jnp.maximum(z - 8, 0)
            core_wait_one(far, 0, far)
            fold(lambda i: kv[far * 4 + i * 2], None, 2, False, False, later=True)

        plus(1, 7)
        minus(0, 7)

        @pl.when(s == 2)
        def _():
            gather_one()

        @pl.when(s == 3)
        def _():
            gather_two()

        @pl.when(s == 5)
        def _():
            expert(1)

        @pl.when(s < 8)
        def _():
            fold_minus()

        return carry

    lax.fori_loop(1, 9, tick, 0)

    @pl.when(z >= 8)
    def _():
        sum_two(1)
        far = jnp.maximum(z - 8, 0)
        core_wait_one(far, 1, NZ)
        for m in range(2):
            out = jnp.dot(kv[far * 4 + 1], weights[m, 0], preferred_element_type=f32)
            acc[m] = acc[m] + (
                out + jnp.dot(kv[far * 4 + 3], weights[m, 1], preferred_element_type=f32)
            )


    @pl.when(z < 8)
    def _():
        sum_two(0)
        sum_two(1)

    for load in loads[11:14]:
        load.wait()
    diff = acc[0] * (1.0 / run_sum[0]) - acc[1] * (lam[...] / run_sum[1])
    mean = jnp.mean(diff * diff, axis=0, keepdims=True)
    head_t = diff * lax.rsqrt(mean + norm_eps)
    for half in range(2):
        head = (head_t[:, half * 128:(half + 1) * 128].T * gain[...]).astype(bf16)
        for i in range(NY):
            for j in range(NX):
                at = (i * NX + j) * COLS
                part = jnp.dot(
                    head, wout[:, at:at + COLS], preferred_element_type=f32
                ).astype(bf16)
                tail[2 * half, i, j] = part[:64]
                tail[2 * half + 1, j, i] = part[64:]
        for g in (2 * half, 2 * half + 1):
            u, v = place[g % 2]
            tail_group(
                0, g, lambda d: tail.at[g, (u + d) % 4], lambda d: tail_in.at[g, d - 1],
                second_peer[g % 2],
            )

    @pl.when(z >= 8)
    def _():
        sum_two(2)
        sum_two(3)

    for g in range(4):
        u, v = place[g % 2]
        tail_three(0, g, tail_in.at[g]).wait_recv()
        for j in range(4):
            t = tail[g, u, j].astype(f32)
            for d in range(3):
                t = t + tail_in[g, d, j].astype(f32)
            tail_mid[g, j] = t.astype(bf16)
        tail_group(
            1, g, lambda d: tail_mid.at[g, (v + d) % 4], lambda d: tail_fin.at[g, d - 1],
            first_peer[g % 2],
        )
        if g == 1:
            @pl.when(z < 8)
            def _():
                sum_two(2)
                sum_two(3)

    most = pl.ds(0, NZ - 1)
    remote(
        ret_send.at[most], ret.at[0, most], ret_sent.at[0], ret_came.at[0], partner
    ).wait_recv()
    back = remote(ret.at[0], ret.at[1], pair_send.at[1], pair_recv.at[1], partner)
    back.start()

    back.wait_recv()
    rows = ret[...].reshape(2 * NZ * PAIR, COLS)
    mixture = jnp.dot(pick[0], rows, preferred_element_type=f32) * spread[0]
    mixture = mixture + jnp.dot(pick[1], rows, preferred_element_type=f32) * spread[1]
    expert_out[...] = mixture.astype(bf16)

    for g in range(4):
        tail_three(1, g, tail_fin.at[g]).wait_recv()
        t = tail_mid[g, place[g % 2][1]].astype(f32)
        for d in range(3):
            t = t + tail_fin[g, d].astype(f32)
        mixed[64 * g:64 * (g + 1)] = t.astype(bf16)

    exch.wait_send()
    back.wait_send()
    remote(z_send.at[most], z_in.at[most], z_sent.at[0], z_came.at[0], partner).wait_send()
    remote(
        ret_send.at[most], ret.at[0, most], ret_sent.at[0], ret_came.at[0], partner
    ).wait_send()
    group_three(0, 0, ag.at[0, few]).wait_send()
    group_three(1, 0, ag.at[few]).wait_send()
    group_three(2, 0, rs_in).wait_send()
    group_three(3, 0, fin).wait_send()
    tail_three(0, 0, tail_in).wait_send()
    tail_three(1, 0, tail_fin).wait_send()

    def sent(way, count):
        if count:
            here = kv.at[pl.ds(0, count)]
            remote(here, here, kv_sent.at[way], core_recv.at[0], partner).wait_send()

    for at in range(NZ):
        @pl.when(z == at)
        def _():
            came_plus = [min(at, 8 - p) for p in range(2)]
            on_plus = [0 if at == NZ - 1 else 1 + min(at, 7 - p) for p in range(2)]
            on_minus = [
                sum((at + s) % NZ <= 6 + p for s in range(7 + p)) for p in range(2)
            ]
            wrapped = [
                sum((at + s) % NZ <= 6 + p and at + s >= NZ for s in range(1, 8 + p))
                for p in range(2)
            ]
            sent(0, sum(on_plus))
            sent(1, sum(on_minus))
            passed = sum(came_plus) + sum(wrapped)

            @pl.when(c == 0)
            def _():
                sent(2, passed + 2)

            @pl.when(c == 1)
            def _():
                sent(2, passed)


def call_kernel(*operands):
    vmem = pl.BlockSpec(memory_space=pltpu.VMEM)
    hbm = pl.BlockSpec(memory_space=pl.ANY)
    n = 4 * PAIR
    h = ROWS // 4
    V = lambda *shape: pltpu.VMEM(shape, bf16)
    F = lambda *shape: pltpu.VMEM(shape, f32)
    D = lambda *shape: pltpu.SemaphoreType.DMA(shape)
    return pl.pallas_call(
        layer_kernel,
        out_shape=(
            pltpu.VMEM((ROWS, COLS), bf16),
            pltpu.VMEM((128, COLS), bf16),
        ),
        in_specs=[hbm] * 14,
        out_specs=(vmem, vmem),
        scratch_shapes=[
            V(ROWS, 256), V(ROWS, 256), V(ROWS, 256),
            F(1, 128), F(ROWS, 128), F(ROWS, 128), F(1, 1), F(1, 256), V(128, 2048), F(1, 2048),
            pltpu.VMEM((2, 128), jnp.int32), F(2, 128),
            V(256, ROWS), V(2, ROWS, ROWS), V(2, NZ, PAIR, COLS), V(2, 128, 2 * NZ * PAIR),
            F(2, 128, 128), V(2, 2, ROWS, ROWS),
            V(4 * NZ, ROWS, ROWS),
            pltpu.VMEM((2, ROWS, ROWS), f32),
            pltpu.VMEM((2, 1, ROWS), f32),
            pltpu.VMEM((2, 1, ROWS), f32),
            V(ROWS, 2048), V(2048, 256), V(2048, 256), V(256, 2048),
            V(NZ, PAIR, COLS), V(NZ, PAIR, COLS), V(NZ, PAIR, COLS),
            V(4, 4, 4, 4, PAIR, COLS), V(4, 4, 4, n, COLS), V(4, 3, 4, n, COLS),
            V(4, 4, n, COLS), V(4, 3, n, COLS),
            V(NZ, PAIR, COLS), V(2, NZ, PAIR, COLS),
            V(4, 4, 4, h, COLS), V(4, 3, 4, h, COLS), V(4, 4, h, COLS), V(4, 3, h, COLS),
            D(NZ, 2), D(NZ + 1), D(3), D(2), D(2), D(1), D(1), D(1), D(1), D(4), D(4, 4), D(2), D(2, 4), D(14),
            pltpu.SemaphoreType.REGULAR((2,)),
        ],
        compiler_params=pltpu.CompilerParams(
            collective_id=0, has_side_effects=True, vmem_limit_bytes=60 * 1024 * 1024
        ),
    )(*operands)


def on_device(
    query_maps, key_maps, value_rows, head_lambda, head_gain, out_weight,
    expert_rows, expert_gain, routes, route_weights, gate_weight, up_weight, down_weight,
):
    turns = rope_base ** (-2.0 * (np.arange(128) % 64) / 128)
    return call_kernel(
        query_maps, key_maps, value_rows, jnp.asarray(turns[None], f32),
        head_lambda.reshape(1, 1), head_gain.reshape(1, -1), out_weight, expert_rows,
        expert_gain.reshape(1, -1), routes.T, route_weights.T,
        gate_weight[0], up_weight[0], down_weight[0],
    )


def solution(mesh):
    placed = (
        P("ep", "tp"),
        P("ep", "tp"),
        P("ep", "tp"),
        P("tp"),
        P(),
        P("tp", None),
        P("ep", None),
        P(),
        P("ep", None),
        P("ep", None),
        P("ep", None, "tp"),
        P("ep", None, "tp"),
        P("ep", "tp", None),
    )
    return jax.shard_map(
        on_device,
        mesh=mesh,
        in_specs=placed,
        out_specs=(P("ep", "tp"), P("ep", "tp")),
        check_vma=False,
    )
```
